128 devices in a mesh: rep: 2 (over z_hi), fs: 32 (over z_lo, y, x), tp: 2 (over core).
Axes of the slice: x: 4, y: 4, z: 4 (z_hi: 2, z_lo: 2; z = z_hi * 2 + z_lo), core: 2. Of those that a mesh axis runs over, the one named last changes fastest.
Arguments:
- resid: bfloat16 [49152, 2048], P(('rep', 'fs', 'tp')), may hold values from -6 to 6
- mix_gain: float32 [2048], replicated, may hold values from 0.1 to 1.9
- query_weight: bfloat16 [2048, 1024], P('fs', 'tp'), may hold values from -0.125 to 0.125
- key_weight: bfloat16 [2048, 1024], P('fs', 'tp'), may hold values from -0.125 to 0.125
- value_weight: bfloat16 [2048, 2048], P('fs', 'tp'), may hold values from -0.125 to 0.125
- head_gain: float32 [2048], P('tp'), may hold values from 0.1 to 1.9
- out_weight: bfloat16 [2048, 2048], P('tp', 'fs'), may hold values from -0.125 to 0.125
- mlp_gain: float32 [2048], replicated, may hold values from 0.1 to 1.9
- gate_weight: bfloat16 [2048, 2816], P('fs', 'tp'), may hold values from -0.125 to 0.125
- up_weight: bfloat16 [2048, 2816], P('fs', 'tp'), may hold values from -0.125 to 0.125
- down_weight: bfloat16 [2816, 2048], P('tp', 'fs'), may hold values from -0.109375 to 0.109375
Outputs:
- layer_out: bfloat16 [49152, 2048], P(('rep', 'fs', 'tp'))
The draws below stay inside these ranges and needn't reach their ends.
All inputs are finite; a program needn't handle non-finite values.
Results may differ from the reference program's by a relative error of at most 0.014.
Values may be sent and summed in bfloat16 or wider, within the bound.
A program may use at most 128 MiB of HBM per device.

```python
import jax
import jax.numpy as jnp
from jax import lax

D = 2048
HEADS = 4
DK = 256
DV = 512
FF = 2816
BLOCK = 128
LEN = 768
TOKENS = 49152
N_TP = 2


def shard_levels(own_key, shape, pieces, least, top_value):
    def one(dim, parts):
        heights = jax.random.uniform(jax.random.fold_in(jax.random.fold_in(own_key, 6), dim), (parts,), jnp.float32, least / len(pieces), top_value / len(pieces))
        return jnp.repeat(jnp.exp(heights), shape[dim] // parts).reshape((-1,) + (1,) * (len(shape) - dim - 1))

    level = one(*pieces[0])
    for cut in pieces[1:]:
        level = level * one(*cut)
    return level


def noise(stream_key, dims, spread, reach, split=(), held_as=jnp.bfloat16):
    level = shard_levels(stream_key, dims, split, -0.22, 0.18) if split else 1.0
    entries = jax.random.normal(stream_key, dims, jnp.float32) * spread * level
    return jnp.minimum(jnp.maximum(entries, -reach), reach).astype(held_as)


def setup_inputs(seed: int = 0) -> dict:
    arg_keys = jax.random.split(jax.random.key(seed), 12)
    resid = noise(arg_keys[0], (TOKENS, D), 1.0, 6.0, ((0, 128),))
    mix_gain = jnp.clip(1.0 + 0.18 * jax.random.normal(arg_keys[1], (D,), jnp.float32), 0.1, 1.9)
    query_weight = noise(arg_keys[2], (D, HEADS * DK), D ** -0.5, 0.125, ((0, 32), (1, 2)))
    key_weight = noise(arg_keys[3], (D, HEADS * DK), D ** -0.5, 0.125, ((0, 32), (1, 2)))
    value_weight = noise(arg_keys[4], (D, HEADS * DV), D ** -0.5, 0.125, ((0, 32), (1, 2)))
    head_gain = jnp.clip(1.0 + 0.18 * jax.random.normal(arg_keys[5], (HEADS * DV,), jnp.float32), 0.1, 1.9)
    out_weight = noise(arg_keys[6], (HEADS * DV, D), (HEADS * DV) ** -0.5, 0.125, ((0, 2), (1, 32)))
    mlp_gain = jnp.clip(1.0 + 0.18 * jax.random.normal(arg_keys[7], (D,), jnp.float32), 0.1, 1.9)
    gate_weight = noise(arg_keys[8], (D, FF), D ** -0.5, 0.125, ((0, 32), (1, 2)))
    up_weight = noise(arg_keys[9], (D, FF), D ** -0.5, 0.125, ((0, 32), (1, 2)))
    down_weight = noise(arg_keys[10], (FF, D), FF ** -0.5, 0.109375, ((0, 2), (1, 32)))
    return {"resid": resid, "mix_gain": mix_gain, "query_weight": query_weight, "key_weight": key_weight, "value_weight": value_weight, "head_gain": head_gain, "out_weight": out_weight, "mlp_gain": mlp_gain, "gate_weight": gate_weight, "up_weight": up_weight, "down_weight": down_weight}


norm_eps = 1e-06
rope_base = 10000.0

def stored(values):
    return lax.optimization_barrier(values.astype(jnp.bfloat16)).astype(jnp.float32)

def rms_scale(values, gain):
    widened = values.astype(jnp.float32)
    scaled = widened * lax.rsqrt(lax.optimization_barrier(jnp.mean(widened * widened, axis=-1, keepdims=True)) + norm_eps)
    return (scaled * gain.astype(jnp.float32)).astype(jnp.bfloat16)

def rotate(vectors):
    length_total = vectors.shape[0]
    half_width = vectors.shape[-1] // 2
    position = jnp.arange(length_total, dtype=jnp.float32)
    inverse = 1.0 / rope_base ** jnp.linspace(0.0, 1.0, half_width, dtype=jnp.float32)
    angle = position[:, None] * inverse[None, :]
    cosine = jnp.cos(angle)[:, None, :]
    sine = jnp.sin(angle)[:, None, :]
    first = vectors[..., :half_width]
    second = vectors[..., half_width:]
    return jnp.concatenate([first * cosine - second * sine, second * cosine + first * sine], axis=-1)

def decay_tables(head_ids, block):
    log_gamma = jnp.log1p(-2.0 ** (-5.0 - 2.0 * head_ids.astype(jnp.float32)))
    offset = jnp.arange(block, dtype=jnp.float32)
    distance = offset[:, None] - offset[None, :]
    inside = jnp.where(distance >= 0, jnp.exp(log_gamma[:, None, None] * jnp.maximum(distance, 0.0)), 0.0)
    query_decay = jnp.exp(log_gamma[:, None] * (offset + 1.0))
    key_decay = jnp.exp(log_gamma[:, None] * (block - 1.0 - offset))
    block_decay = jnp.exp(log_gamma * block)
    return (inside, query_decay, key_decay, block_decay)

def retain(queries, keys, values, head_ids, block):
    length_total, heads, key_width = queries.shape
    value_width = values.shape[-1]
    count = length_total // block
    inside, query_decay, key_decay, block_decay = decay_tables(head_ids, block)

    def blocks(tensor):
        return tensor.reshape(count, block, heads, tensor.shape[-1]).transpose(0, 2, 1, 3)

    def advance(memory, inputs):
        query_tile_rows, key_tile_rows, value_block = inputs
        query_widened = query_tile_rows.astype(jnp.float32)
        value_wide = value_block.astype(jnp.float32)
        attention_scores = jnp.einsum('zvf,zjf->zvj', query_widened, key_tile_rows.astype(jnp.float32))
        weights = stored(attention_scores * inside)
        within = jnp.einsum('hlm,hmv->hlv', weights, value_wide)
        carried = jnp.einsum('hld,hdv->hlv', query_widened, stored(memory)) * query_decay[:, :, None]
        weighted_keys = stored(key_tile_rows.astype(jnp.float32) * key_decay[:, :, None])
        memory = memory * block_decay[:, None, None] + jnp.einsum('hld,hlv->hdv', weighted_keys, value_wide)
        return (memory, within + carried)
    start_state = jnp.zeros((heads, key_width, value_width), jnp.float32)
    _, outputs = lax.scan(advance, start_state, (blocks(queries), blocks(keys), blocks(values)))
    return outputs.transpose(0, 2, 1, 3).reshape(length_total, heads, value_width)

def head_scale(retained, gain):
    scaled = retained * lax.rsqrt(lax.optimization_barrier(jnp.mean(retained * retained, axis=-1, keepdims=True)) + norm_eps)
    return (scaled.reshape(retained.shape[0], -1) * gain.astype(jnp.float32)).astype(jnp.bfloat16)

def reference(resid, mix_gain, query_weight, key_weight, value_weight, head_gain, out_weight, mlp_gain, gate_weight, up_weight, down_weight):
    head_ids = jnp.arange(HEADS, dtype=jnp.int32)
    head_share = HEADS * DV // N_TP
    unit_share = FF // N_TP

    def single_sequence(token_rows):
        normed = rms_scale(token_rows, mix_gain)
        queries = stored(jnp.dot(normed, query_weight, preferred_element_type=jnp.float32)).reshape(LEN, HEADS, DK)
        keys = stored(jnp.dot(normed, key_weight, preferred_element_type=jnp.float32)).reshape(LEN, HEADS, DK)
        values = jnp.dot(normed, value_weight, preferred_element_type=jnp.float32).astype(jnp.bfloat16)
        values = values.reshape(LEN, HEADS, DV)
        query_rot = rotate(queries).astype(jnp.bfloat16)
        key_rot = (rotate(keys) * DK ** (-0.5)).astype(jnp.bfloat16)
        retained = retain(query_rot, key_rot, values, head_ids, BLOCK)
        head_out = head_scale(retained, head_gain)
        mixer_sum = jnp.zeros((LEN, D), jnp.float32)
        for group in range(N_TP):
            lower = group * head_share
            partial_sum = jnp.dot(head_out[:, lower:lower + head_share], out_weight[lower:lower + head_share], preferred_element_type=jnp.float32)
            mixer_sum = mixer_sum + stored(partial_sum)
        middle = (token_rows.astype(jnp.float32) + mixer_sum).astype(jnp.bfloat16)
        normed_mlp = rms_scale(middle, mlp_gain)
        gate = jnp.dot(normed_mlp, gate_weight, preferred_element_type=jnp.float32)
        upward = jnp.dot(normed_mlp, up_weight, preferred_element_type=jnp.float32)
        hidden_units = (jax.nn.silu(gate) * upward).astype(jnp.bfloat16)
        mlp_sum = jnp.zeros((LEN, D), jnp.float32)
        for group in range(N_TP):
            lower = group * unit_share
            partial_sum = jnp.dot(hidden_units[:, lower:lower + unit_share], down_weight[lower:lower + unit_share], preferred_element_type=jnp.float32)
            mlp_sum = mlp_sum + stored(partial_sum)
        return (middle.astype(jnp.float32) + mlp_sum).astype(jnp.bfloat16)
    sequences = resid.reshape(TOKENS // LEN, LEN, D)
    return lax.map(single_sequence, sequences).reshape(TOKENS, D)
```

```python
import heapq

import jax
import jax.numpy as jnp
from jax import lax
from jax.experimental import pallas as pl
from jax.experimental.pallas import tpu as pltpu
from jax.sharding import Mesh
from jax.sharding import PartitionSpec as P

DK = 256
DV = 512
BLOCK = 128
FS = ("fs_0", "fs_1", "fs_2")
REP_FS_TP = ("rep", "fs_0", "fs_1", "fs_2", "tp")
MESH_ID = pl.DeviceIdType.MESH
PIECES = 4
ROWS = 64
PIECE_ROWS = ROWS // PIECES
WIDTHS = (2048, 1024, 2816, 1408)
OFFSETS = [(z, y, x) for z in range(2) for y in range(4) for x in range(4)]
ROOT = (0, 0, 0)

norm_eps = 1e-06
rope_base = 10000.0


def parent(piece, offset):
    z, y, x = offset
    for axis in ("zxy", "zyx", "xzy", "yzx")[piece]:
        if axis == "z" and z:
            return 4 + (x + y + piece) % 2, (0, y, x)
        if axis == "x" and x:
            up = x == 1 or (x == 2 and (piece == 1 or (piece in (0, 2) and (y + z + piece // 2) % 2 == 0)))
            return (0, (z, y, x - 1)) if up else (1, (z, y, (x + 1) % 4))
        if axis == "y" and y:
            up = y == 1 or (y == 2 and (piece == 0 or (piece in (1, 3) and (x + z) % 2 == 0)))
            return (2, (z, y - 1, x)) if up else (3, (z, (y + 1) % 4, x))
    return None


def copy_order(widths, rate=46.6e3, latency=2.2, lead=3.0):
    kids = {}
    for piece in range(PIECES):
        for offset in OFFSETS[1:]:
            d, above = parent(piece, offset)
            kids.setdefault((piece, above), []).append((offset, d))

    def depth(piece, offset):
        return max([0] + [1 + depth(piece, c) for c, _ in kids.get((piece, offset), [])])

    ready = [[] for _ in range(6)]
    free = [0.0] * 6
    arrival = {}
    events = []
    sends = []
    for array in range(len(widths)):
        for piece in range(PIECES):
            heapq.heappush(events, (0.0, 0, (array, piece, ROOT)))
    while events:
        now = events[0][0]
        while events and events[0][0] <= now + 1e-9:
            _, kind, item = heapq.heappop(events)
            if kind == 0:
                arrival[item] = now
                array, piece, offset = item
                for child, d in kids.get((piece, offset), []):
                    heapq.heappush(ready[d], (array, -depth(piece, child), piece, child, offset))
        for d in range(6):
            if free[d] <= now + 1e-9 and ready[d]:
                array, _, piece, child, offset = heapq.heappop(ready[d])
                wire = widths[array] * 2 * PIECE_ROWS / rate
                issue = max(arrival[array, piece, offset], now - lead)
                sends.append((issue, now, d, array, piece, offset, child))
                free[d] = now + wire
                heapq.heappush(events, (now + wire, 1, (0, 0, ROOT)))
                heapq.heappush(events, (now + wire + latency, 0, (array, piece, child)))
    sends.sort()
    return sends, arrival


SENDS, ARRIVAL = copy_order(WIDTHS)


def slot_of(array, piece, offset):
    return (array * PIECES + piece) * len(OFFSETS) + OFFSETS.index(offset)


def gather_kernel(q_ref, k_ref, v_ref, o_ref, g_ref, u_ref, d_ref, qkv, out, mlp, down, recv, send, local):
    fulls = (qkv, out, mlp, down)
    rep, lo, my, mx, core = (lax.axis_index(a) for a in REP_FS_TP)
    z = rep * 2 + lo
    zu, zd = lax.rem(z + 1, 4), lax.rem(z + 3, 4)
    peers = (
        {"fs_2": lax.rem(mx + 1, 4)},
        {"fs_2": lax.rem(mx + 3, 4)},
        {"fs_1": lax.rem(my + 1, 4)},
        {"fs_1": lax.rem(my + 3, 4)},
        {"rep": zu // 2, "fs_0": lax.rem(zu, 2)},
        {"rep": zd // 2, "fs_0": lax.rem(zd, 2)},
    )
    barrier = pltpu.get_barrier_semaphore()
    for peer in peers:
        pl.semaphore_signal(barrier, inc=1, device_id=peer, device_id_type=MESH_ID)

    def base(offset):
        oz, oy, ox = offset
        owner = (lax.rem(lo + oz, 2) * 4 + lax.rem(my + 4 - oy, 4)) * 4 + lax.rem(mx + 4 - ox, 4)
        return owner * ROWS

    mine = pl.multiple_of(base(ROOT), ROWS)
    own = pl.ds(mine, ROWS)
    fills = [
        (q_ref, qkv.at[own, pl.ds(0, 512)]),
        (k_ref, qkv.at[own, pl.ds(512, 512)]),
        (v_ref, qkv.at[own, pl.ds(1024, 1024)]),
        (o_ref, out.at[own, :]),
        (g_ref, mlp.at[own, pl.ds(0, 1408)]),
        (u_ref, mlp.at[own, pl.ds(1408, 1408)]),
        (d_ref, down.at[own, :]),
    ]
    fills = [pltpu.make_async_copy(a, b, local.at[i]) for i, (a, b) in enumerate(fills)]
    for fill in fills:
        fill.start()
    for fill in fills:
        fill.wait()
    pl.semaphore_wait(barrier, 6)

    def chunk(array, piece, offset):
        start = pl.multiple_of(base(offset) + piece * PIECE_ROWS, PIECE_ROWS)
        return fulls[array].at[pl.ds(start, PIECE_ROWS), :]

    waited = set()

    def arrive(array, piece, offset):
        if offset == ROOT or (array, piece, offset) in waited:
            return
        waited.add((array, piece, offset))
        here = chunk(array, piece, offset)
        pltpu.make_async_copy(here, here, recv.at[slot_of(array, piece, offset)]).wait()

    for _, _, d, array, piece, offset, child in SENDS:
        arrive(array, piece, offset)
        here = chunk(array, piece, offset)
        pltpu.make_async_remote_copy(
            src_ref=here,
            dst_ref=here,
            send_sem=send.at[array],
            recv_sem=recv.at[slot_of(array, piece, child)],
            device_id=peers[d],
            device_id_type=MESH_ID,
        ).start()
    for array, piece, offset in sorted(ARRIVAL, key=ARRIVAL.get):
        arrive(array, piece, offset)
    for array, full in enumerate(fulls):
        sent = full.at[pl.ds(0, 31 * ROWS), :]
        pltpu.make_async_copy(sent, sent, send.at[array]).wait()


def gather_all(query, key, value, out_t, gate, up, down_t):
    anywhere = pl.BlockSpec(memory_space=pl.ANY)
    return pl.pallas_call(
        gather_kernel,
        out_shape=[jax.ShapeDtypeStruct((32 * ROWS, w), jnp.bfloat16) for w in WIDTHS],
        in_specs=[anywhere] * 7,
        out_specs=[pl.BlockSpec(memory_space=pltpu.VMEM)] * 4,
        scratch_shapes=[
            pltpu.SemaphoreType.DMA((4 * PIECES * len(OFFSETS),)),
            pltpu.SemaphoreType.DMA((4,)),
            pltpu.SemaphoreType.DMA((7,)),
        ],
        compiler_params=pltpu.CompilerParams(
            collective_id=0, has_side_effects=True, vmem_limit_bytes=56 << 20
        ),
    )(query, key, value, out_t, gate, up, down_t)


def cut_along(shard, dim, peers):
    lengths = shard.shape
    pieces = shard.reshape(*lengths[:dim], peers, lengths[dim] // peers, *lengths[dim + 1 :])
    return jnp.moveaxis(pieces, dim, 0)


def sum_at_owner(shard, axis, dim):
    pieces = cut_along(shard, dim, lax.axis_size(axis))
    arrived = lax.all_to_all(pieces, axis, split_axis=0, concat_axis=0, tiled=True)
    return arrived.astype(jnp.float32).sum(axis=0)


def rms_scale(values, gain):
    widened = values.astype(jnp.float32)
    scaled = widened * lax.rsqrt(jnp.mean(widened * widened, axis=-1, keepdims=True) + norm_eps)
    return (scaled * gain).astype(jnp.bfloat16)


def rotate(vectors):
    length_total = vectors.shape[0]
    half_width = vectors.shape[-1] // 2
    position = jnp.arange(length_total, dtype=jnp.float32)
    inverse = 1.0 / rope_base ** jnp.linspace(0.0, 1.0, half_width, dtype=jnp.float32)
    angle = position[:, None] * inverse[None, :]
    cosine = jnp.cos(angle)[:, None, :]
    sine = jnp.sin(angle)[:, None, :]
    first = vectors[..., :half_width]
    second = vectors[..., half_width:]
    return jnp.concatenate(
        [first * cosine - second * sine, second * cosine + first * sine], axis=-1
    )


def decay_tables(head_ids, block):
    log_gamma = jnp.log1p(-(2.0 ** (-5.0 - 2.0 * head_ids.astype(jnp.float32))))
    offset = jnp.arange(block, dtype=jnp.float32)
    distance = offset[:, None] - offset[None, :]
    inside = jnp.where(
        distance >= 0, jnp.exp(log_gamma[:, None, None] * jnp.maximum(distance, 0.0)), 0.0
    )
    query_decay = jnp.exp(log_gamma[:, None] * (offset + 1.0))
    key_decay = jnp.exp(log_gamma[:, None] * (block - 1.0 - offset))
    block_decay = jnp.exp(log_gamma * block)
    return (inside, query_decay, key_decay, block_decay)


def retain(queries, keys, values, head_ids, block):
    length_total, heads, key_width = queries.shape
    value_width = values.shape[-1]
    count = length_total // block
    inside, query_decay, key_decay, block_decay = decay_tables(head_ids, block)

    def blocks(tensor):
        return tensor.reshape(count, block, heads, tensor.shape[-1]).transpose(0, 2, 1, 3)

    def advance(memory, inputs):
        query_tile_rows, key_tile_rows, value_block = inputs
        attention_scores = jnp.einsum(
            "zvf,zjf->zvj", query_tile_rows, key_tile_rows, preferred_element_type=jnp.float32
        )
        weights = (attention_scores * inside).astype(jnp.bfloat16)
        within = jnp.einsum(
            "hlm,hmv->hlv", weights, value_block, preferred_element_type=jnp.float32
        )
        carried = (
            jnp.einsum(
                "hld,hdv->hlv",
                query_tile_rows,
                memory.astype(jnp.bfloat16),
                preferred_element_type=jnp.float32,
            )
            * query_decay[:, :, None]
        )
        weighted_keys = (key_tile_rows.astype(jnp.float32) * key_decay[:, :, None]).astype(
            jnp.bfloat16
        )
        memory = memory * block_decay[:, None, None] + jnp.einsum(
            "hld,hlv->hdv", weighted_keys, value_block, preferred_element_type=jnp.float32
        )
        return (memory, within + carried)

    start_state = jnp.zeros((heads, key_width, value_width), jnp.float32)
    _, outputs = lax.scan(advance, start_state, (blocks(queries), blocks(keys), blocks(values)))
    return outputs.transpose(0, 2, 1, 3).reshape(length_total, heads, value_width)


def head_scale(retained, gain):
    scaled = retained * lax.rsqrt(jnp.mean(retained * retained, axis=-1, keepdims=True) + norm_eps)
    return (scaled.reshape(retained.shape[0], -1) * gain).astype(jnp.bfloat16)


def shards(
    resid,
    mix_gain,
    query_weight,
    key_weight,
    value_weight,
    head_gain,
    out_weight,
    mlp_gain,
    gate_weight,
    up_weight,
    down_weight,
):
    token_rows = resid.shape[0]
    length_total = token_rows * lax.axis_size("tp")
    key_cols = query_weight.shape[1]
    heads_here = key_cols // DK
    normed = rms_scale(resid, mix_gain)
    mixer_full, out_full, mlp_full, down_full = gather_all(
        query_weight, key_weight, value_weight, out_weight.T, gate_weight, up_weight, down_weight.T
    )
    projected = jnp.dot(
        lax.all_gather(normed, "tp", axis=0, tiled=True),
        mixer_full,
        preferred_element_type=jnp.float32,
    ).astype(jnp.bfloat16)
    queries = projected[:, :key_cols].astype(jnp.float32).reshape(length_total, heads_here, DK)
    keys = (
        projected[:, key_cols : 2 * key_cols]
        .astype(jnp.float32)
        .reshape(length_total, heads_here, DK)
    )
    values = projected[:, 2 * key_cols :].reshape(length_total, heads_here, DV)
    query_rot = rotate(queries).astype(jnp.bfloat16)
    key_rot = (rotate(keys) * DK ** (-0.5)).astype(jnp.bfloat16)
    head_ids = lax.axis_index("tp") * heads_here + jnp.arange(heads_here, dtype=jnp.int32)
    retained = retain(query_rot, key_rot, values, head_ids, BLOCK)
    head_out = head_scale(retained, head_gain)
    selected = head_out
    mixer_sum = sum_at_owner(
        lax.dot_general(
            selected, out_full, (((1,), (1,)), ((), ())), preferred_element_type=jnp.float32
        ).astype(jnp.bfloat16),
        "tp",
        0,
    )
    middle = (resid.astype(jnp.float32) + mixer_sum).astype(jnp.bfloat16)
    normed_mlp = rms_scale(middle, mlp_gain)
    local_units = gate_weight.shape[1]
    both = jnp.dot(
        lax.all_gather(normed_mlp, "tp", axis=0, tiled=True),
        mlp_full,
        preferred_element_type=jnp.float32,
    )
    hidden_units = (jax.nn.silu(both[:, :local_units]) * both[:, local_units:]).astype(jnp.bfloat16)
    selected = hidden_units
    mlp_sum = sum_at_owner(
        lax.dot_general(
            selected, down_full, (((1,), (1,)), ((), ())), preferred_element_type=jnp.float32
        ).astype(jnp.bfloat16),
        "tp",
        0,
    )
    return (middle.astype(jnp.float32) + mlp_sum).astype(jnp.bfloat16)


def solution(mesh):
    torus = Mesh(
        mesh.devices.reshape(mesh.shape["rep"], 2, 4, 4, mesh.shape["tp"]),
        ("rep", "fs_0", "fs_1", "fs_2", "tp"),
    )
    return jax.shard_map(
        shards,
        mesh=torus,
        in_specs=(
            P(REP_FS_TP, None),
            P(),
            P(FS, "tp"),
            P(FS, "tp"),
            P(FS, "tp"),
            P("tp"),
            P("tp", FS),
            P(),
            P(FS, "tp"),
            P(FS, "tp"),
            P("tp", FS),
        ),
        out_specs=P(REP_FS_TP, None),
        check_vma=False,
    )
```

```python
import heapq

import jax
import jax.numpy as jnp
import numpy as np
from jax import lax
from jax.experimental import pallas as pl
from jax.experimental.pallas import tpu as pltpu
from jax.sharding import Mesh
from jax.sharding import PartitionSpec as P

D = 2048
DK = 256
DV = 512
BLOCK = 128
LEN = 768
HALF = LEN // 2
UNITS = 1408
FS = ("fs_0", "fs_1", "fs_2")
REP_FS_TP = ("rep", "fs_0", "fs_1", "fs_2", "tp")
MESH_ID = pl.DeviceIdType.MESH
PIECES = 4
ROWS = 64
PIECE_ROWS = ROWS // PIECES
ARRAYS = ((0, 0, 1024), (0, 1024, 1024), (1, 0, 1024), (2, 0, 1536), (2, 1536, 1280), (3, 0, UNITS))
WIDTHS = tuple(width for _, _, width in ARRAYS)
LAST = len(ARRAYS) - 1
OFFSETS = [(z, y, x) for z in range(2) for y in range(4) for x in range(4)]
GROUPS = [(z, y) for z in range(2) for y in range(4)]
ROOT = (0, 0, 0)
F32 = jnp.float32
BF16 = jnp.bfloat16

norm_eps = 1e-06
rope_base = 10000.0


def parent(piece, offset):
    z, y, x = offset
    for axis in ("zxy", "zyx", "xzy", "yzx")[piece]:
        if axis == "z" and z:
            return 4 + (x + y + piece) % 2, (0, y, x)
        if axis == "x" and x:
            up = x == 1 or (x == 2 and (piece == 1 or (piece in (0, 2) and (y + z + piece // 2) % 2 == 0)))
            return (0, (z, y, x - 1)) if up else (1, (z, y, (x + 1) % 4))
        if axis == "y" and y:
            up = y == 1 or (y == 2 and (piece == 0 or (piece in (1, 3) and (x + z) % 2 == 0)))
            return (2, (z, y - 1, x)) if up else (3, (z, (y + 1) % 4, x))
    return None


def compute_steps():
    steps = [("norm", (0,), (), 2.0), ("norm", (1,), (), 2.0)]
    steps += [("proj", (j,), (0 if j < 4 else 1,), 1.3) for j in range(8)]
    steps += [("ret", (t, h), (), 1.2) for t in range(LEN // BLOCK) for h in range(2)]
    steps += [("out", (1, j), (2,), 0.5) for j in range(8)]
    steps += [("out", (0, j), (), 0.5) for j in range(8)]
    steps += [("mid", (r,), (), 1.0) for r in range(4)]
    steps += [("trade", (), (), 3.0)]
    steps += [("mlp", (j,), (3 if j < 6 else 4,), 1.5) for j in range(11)]
    steps += [("down", (g,), (("g", g),), 1.2) for g in range(8)]
    return steps


def program_order(steps, rate=47.0e3, latency=2.2, lead=8.0, spare=2.5):
    kids = {}
    for piece in range(PIECES):
        for offset in OFFSETS[1:]:
            d, above = parent(piece, offset)
            kids.setdefault((piece, above), []).append((offset, d))

    def depth(piece, offset):
        return max([0] + [1 + depth(piece, c) for c, _ in kids.get((piece, offset), [])])

    def rank(array, piece, child):
        if array == LAST:
            return (array, GROUPS.index(child[:2]), -depth(piece, child))
        return (array, 0, -depth(piece, child))

    def needs(dep):
        if isinstance(dep, tuple):
            return [(LAST, p, o) for p in range(PIECES) for o in OFFSETS if o[:2] == GROUPS[dep[1]]]
        return [(dep, p, o) for p in range(PIECES) for o in OFFSETS]

    ready = [[] for _ in range(6)]
    free = [0.0] * 6
    coming, arrival = [], {}
    for array in range(len(WIDTHS)):
        for piece in range(PIECES):
            heapq.heappush(coming, (2.0, (array, piece, ROOT)))
    left = [PIECES * len(OFFSETS)] * len(WIDTHS)
    order, now, todo = [], 0.0, list(steps)

    def room(d):
        early = ready[d][0][0][0] <= min(a for a in range(len(WIDTHS)) if left[a])
        return lead if early else spare

    while todo or coming or any(ready):
        while coming and coming[0][0] <= now + 1e-9:
            at, item = heapq.heappop(coming)
            arrival[item] = at
            array, piece, offset = item
            left[array] -= 1
            for child, d in kids.get((piece, offset), []):
                heapq.heappush(ready[d], (rank(array, piece, child), piece, child, offset))
        issued = False
        for d in range(6):
            while ready[d] and free[d] - now < room(d):
                (array, *_), piece, child, offset = heapq.heappop(ready[d])
                free[d] = max(free[d], now) + WIDTHS[array] * 2 * PIECE_ROWS / rate
                heapq.heappush(coming, (free[d] + latency, (array, piece, child)))
                order.append(("send", now, (d, array, piece, offset, child)))
                now += 0.03
                issued = True
        if issued:
            continue
        if todo:
            name, args, deps, cost = todo[0]
            wanted = [c for dep in deps for c in needs(dep)]
            if all(c in arrival for c in wanted):
                wanted.sort(key=lambda c: (arrival[c], c))
                order.append((name, now, (args, wanted)))
                now += cost
                todo.pop(0)
                continue
        nexts = [free[d] - room(d) + 1e-3 for d in range(6) if ready[d]]
        if coming:
            nexts.append(coming[0][0])
        now = max(now, min(nexts))
    return order, arrival, now, max(free)


STEPS = compute_steps()
ORDER, ARRIVAL, _, _ = program_order(STEPS)


def tables():
    position = np.arange(LEN, dtype=np.float32)
    inverse = np.float32(1.0) / np.float32(rope_base) ** np.linspace(0.0, 1.0, DK // 2, dtype=np.float32)
    angle = position[:, None] * inverse[None, :]
    log_gamma = np.log1p(-(2.0 ** (-5.0 - 2.0 * np.arange(4))))
    offset = np.arange(BLOCK)
    distance = offset[:, None] - offset[None, :]
    inside = np.where(distance >= 0, np.exp(log_gamma[:, None, None] * np.maximum(distance, 0)), 0.0)
    query_decay = np.exp(log_gamma[:, None] * (offset + 1.0))
    key_decay = np.exp(log_gamma[:, None] * (BLOCK - 1.0 - offset))
    wide = np.ones((1, 1, BLOCK))
    found = (np.cos(angle), np.sin(angle), inside, query_decay[:, :, None] * wide, key_decay[:, :, None] * wide)
    return tuple(jnp.asarray(t.astype(np.float32)) for t in found)


def layer_kernel(
    resid, mix_gain, q_ref, k_ref, v_ref, head_gain, o_ref, mlp_gain, g_ref, u_ref, d_ref,
    cosine, sine, inside, query_decay, key_decay,
    result,
    wq, wo, wm, wd, rows_in, normed, proj, heads, state, hidden, keep, give, take, keep2, give2, take2,
    recv, send, local, swap_send, swap_recv, put,
):
    buffers = (wq, wo, wm, wd)
    rep, lo, my, mx, core = (lax.axis_index(a) for a in REP_FS_TP)
    z = rep * 2 + lo
    zu, zd = lax.rem(z + 1, 4), lax.rem(z + 3, 4)
    peers = (
        {"fs_2": lax.rem(mx + 1, 4)},
        {"fs_2": lax.rem(mx + 3, 4)},
        {"fs_1": lax.rem(my + 1, 4)},
        {"fs_1": lax.rem(my + 3, 4)},
        {"rep": zu // 2, "fs_0": lax.rem(zu, 2)},
        {"rep": zd // 2, "fs_0": lax.rem(zd, 2)},
    )
    partner = {"tp": 1 - core}
    barrier = pltpu.get_barrier_semaphore()
    for peer in peers + (partner,):
        pl.semaphore_signal(barrier, inc=1, device_id=peer, device_id_type=MESH_ID)

    def base(offset):
        oz, oy, ox = offset
        owner = (lax.rem(lo + oz, 2) * 4 + lax.rem(my + 4 - oy, 4)) * 4 + lax.rem(mx + 4 - ox, 4)
        return owner * ROWS

    own = pl.ds(pl.multiple_of(base(ROOT), ROWS), ROWS)
    mine = pl.multiple_of(core * HALF, HALF)
    other = pl.multiple_of(HALF - core * HALF, HALF)
    half = (mine, other)

    def shard(array):
        buffer, first, width = ARRAYS[array]
        return buffers[buffer].at[own, pl.ds(first, width)]

    parts = {
        0: [(q_ref, wq.at[own, pl.ds(0, 512)]), (k_ref, wq.at[own, pl.ds(512, 512)])],
        1: [(v_ref, wq.at[own, pl.ds(1024, 1024)])],
        2: [(o_ref, wo.at[own, :])],
        3: [],
        4: [],
        5: [(d_ref, wd.at[own, :])],
    }
    for j in range(11):
        for which, ref in enumerate((g_ref, u_ref)):
            there = wm.at[own, pl.ds(256 * j + 128 * which, 128)]
            parts[3 if j < 6 else 4].append((ref.at[:, pl.ds(128 * j, 128)], there))
    for array in range(len(ARRAYS)):
        for source, there in parts[array]:
            pltpu.make_async_copy(source, there, local.at[array]).start()
    fill = pltpu.make_async_copy(resid, rows_in.at[pl.ds(mine, HALF), :], local.at[len(ARRAYS)])
    fill.start()
    pl.semaphore_wait(barrier, 7)

    def swap(source, there, slot):
        return pltpu.make_async_remote_copy(
            src_ref=source,
            dst_ref=there,
            send_sem=swap_send.at[slot],
            recv_sem=swap_recv.at[slot],
            device_id=partner,
            device_id_type=MESH_ID,
        )

    swaps = {0: swap(resid, rows_in.at[pl.ds(mine, HALF), :], 0)}
    swaps[0].start()

    def chunk(array, piece, offset):
        buffer, first, width = ARRAYS[array]
        start = pl.multiple_of(base(offset) + piece * PIECE_ROWS, PIECE_ROWS)
        return buffers[buffer].at[pl.ds(start, PIECE_ROWS), pl.ds(first, width)]

    def slot_of(array, piece, offset):
        return (array * PIECES + piece) * len(OFFSETS) + OFFSETS.index(offset)

    waited = set()

    def arrive(array, piece, offset):
        key = (array,) if offset == ROOT else (array, piece, offset)
        if key in waited:
            return
        waited.add(key)
        if offset == ROOT:
            pltpu.make_async_copy(shard(array), shard(array), local.at[array]).wait()
        else:
            here = chunk(array, piece, offset)
            pltpu.make_async_copy(here, here, recv.at[slot_of(array, piece, offset)]).wait()

    def norm_rows(source, gain, start, count):
        def some(i, _):
            rows = pl.ds(pl.multiple_of(start + i * 32, 32), 32)
            wide = source[rows, :].astype(F32)
            scaled = wide * lax.rsqrt(jnp.mean(wide * wide, axis=-1, keepdims=True) + norm_eps)
            normed[rows, :] = (scaled * gain[...]).astype(BF16)

        lax.fori_loop(0, count // 32, some, None)

    def norm(which):
        if which == 0:
            fill.wait()
        else:
            swaps[0].wait()
        norm_rows(rows_in, mix_gain, half[which], HALF)

    def project(j):
        def some(i, _):
            rows = pl.ds(pl.multiple_of(i * HALF, HALF), HALF)
            columns = pl.ds(256 * j, 256)
            found = jnp.dot(normed[rows, :], wq[:, columns], preferred_element_type=F32).astype(BF16)
            if j < 4:
                wide = found.astype(F32)
                first, second = wide[:, :128], wide[:, 128:]
                c, s = cosine[rows, :], sine[rows, :]
                turned = jnp.concatenate([first * c - second * s, second * c + first * s], axis=1)
                if j >= 2:
                    turned = turned * DK**-0.5
                found = turned.astype(BF16)
            proj[rows, columns] = found

        lax.fori_loop(0, 2, some, None)

    def retain(t, h):
        rows = pl.ds(t * BLOCK, BLOCK)
        head = core * 2 + h
        queries = proj[rows, pl.ds(DK * h, DK)]
        keys = proj[rows, pl.ds(2 * DK + DK * h, DK)]
        values = proj[rows, pl.ds(4 * DK + DV * h, DV)]
        decay = query_decay[head]
        scores = lax.dot_general(queries, keys, (((1,), (1,)), ((), ())), preferred_element_type=F32)
        weights = (scores * inside[head]).astype(BF16)
        found = jnp.dot(weights, values, preferred_element_type=F32)
        if t > 0:
            carried = jnp.dot(queries, state[h].astype(BF16), preferred_element_type=F32)
            found = found + carried * jnp.concatenate([decay] * 4, axis=1)
        if t < LEN // BLOCK - 1:
            fade = key_decay[head]
            faded = (keys.astype(F32) * jnp.concatenate([fade] * 2, axis=1)).astype(BF16)
            fresh = lax.dot_general(faded, values, (((0,), (0,)), ((), ())), preferred_element_type=F32)
            if t > 0:
                last = query_decay[head, BLOCK - 1 : BLOCK, :]
                fresh = state[h] * jnp.concatenate([last] * 4, axis=1) + fresh
            state[h] = fresh
        columns = pl.ds(DV * h, DV)
        scaled = found * lax.rsqrt(jnp.mean(found * found, axis=-1, keepdims=True) + norm_eps)
        heads[rows, columns] = (scaled * head_gain[:, columns]).astype(BF16)

    def give_heads(which, j):
        columns = pl.ds(256 * j, 256)
        share = lax.dot_general(
            heads[pl.ds(half[which], HALF), :], wo[columns, :], (((1,), (1,)), ((), ())), preferred_element_type=F32
        ).astype(BF16)
        (give if which else keep)[:, columns] = share
        if (which, j) == (0, 0):
            swaps[1] = swap(give, take, 1)
            swaps[1].start()

    def middle(r):
        if r == 0:
            swaps[1].wait()
        count = HALF // 4

        def some(i, _):
            here = pl.ds(pl.multiple_of(r * count + i * 32, 32), 32)
            rows = pl.ds(pl.multiple_of(mine + r * count + i * 32, 32), 32)
            added = keep[here, :].astype(F32) + take[here, :].astype(F32)
            rows_in[rows, :] = (rows_in[rows, :].astype(F32) + added).astype(BF16)

        lax.fori_loop(0, count // 32, some, None)
        norm_rows(rows_in, mlp_gain, mine + r * count, count)

    def trade():
        rows = pl.ds(mine, HALF)
        swaps[2] = swap(normed.at[rows, :], normed.at[rows, :], 2)
        swaps[2].start()
        swaps[2].wait()

    def expand(j):
        def some(i, _):
            rows = pl.ds(pl.multiple_of(i * HALF, HALF), HALF)
            both = jnp.dot(normed[rows, :], wm[:, pl.ds(256 * j, 256)], preferred_element_type=F32)
            hidden[rows, pl.ds(128 * j, 128)] = (jax.nn.silu(both[:, :128]) * both[:, 128:]).astype(BF16)

        lax.fori_loop(0, 2, some, None)

    blocks = {}

    def contract(g):
        oz, oy = GROUPS[g]
        block = lax.rem(lo + oz, 2) * 4 + lax.rem(my + 4 - oy, 4)
        blocks[g] = block
        columns = wd[pl.ds(pl.multiple_of(block * 256, 256), 256), :]
        for which in (1, 0):
            share = lax.dot_general(
                hidden[pl.ds(half[which], HALF), :], columns, (((1,), (1,)), ((), ())), preferred_element_type=F32
            ).astype(BF16)
            (give2 if which else keep2)[block] = share
        swaps[3 + g] = swap(give2.at[block], take2.at[block], 3 + g)
        swaps[3 + g].start()

    def writing(g):
        place = result.at[:, pl.ds(pl.multiple_of(blocks[g] * 256, 256), 256)]
        return pltpu.make_async_copy(keep2.at[blocks[g]], place, put.at[g])

    def finish(g):
        swaps[3 + g].wait()
        block = blocks[g]

        def some(i, _):
            here = pl.ds(pl.multiple_of(i * 96, 32), 96)
            rows = pl.ds(pl.multiple_of(mine + i * 96, 32), 96)
            columns = pl.ds(pl.multiple_of(block * 256, 256), 256)
            added = keep2[block, here, :].astype(F32) + take2[block, here, :].astype(F32)
            keep2[block, here, :] = (rows_in[rows, columns].astype(F32) + added).astype(BF16)

        lax.fori_loop(0, HALF // 96, some, None)
        writing(g).start()

    def down(g):
        contract(g)
        if g > 0:
            finish(g - 1)

    run = {
        "norm": norm, "proj": project, "ret": retain, "out": give_heads,
        "mid": middle, "trade": trade, "mlp": expand, "down": down,
    }
    for name, _, what in ORDER:
        if name == "send":
            d, array, piece, offset, child = what
            arrive(array, piece, offset)
            here = chunk(array, piece, offset)
            pltpu.make_async_remote_copy(
                src_ref=here,
                dst_ref=here,
                send_sem=send.at[array],
                recv_sem=recv.at[slot_of(array, piece, child)],
                device_id=peers[d],
                device_id_type=MESH_ID,
            ).start()
        else:
            args, wanted = what
            for item in wanted:
                arrive(*item)
            run[name](*args)
    finish(len(GROUPS) - 1)
    for array, (buffer, first, width) in enumerate(ARRAYS):
        sent = buffers[buffer].at[pl.ds(0, 31 * ROWS), pl.ds(first, width)]
        pltpu.make_async_copy(sent, sent, send.at[array]).wait()
    for g in range(len(GROUPS)):
        writing(g).wait()


def shards(
    resid, mix_gain, query_weight, key_weight, value_weight, head_gain, out_weight, mlp_gain,
    gate_weight, up_weight, down_weight,
):
    anywhere = pl.BlockSpec(memory_space=pl.ANY)
    inside = pl.BlockSpec(memory_space=pltpu.VMEM)
    return pl.pallas_call(
        layer_kernel,
        out_shape=jax.ShapeDtypeStruct((HALF, D), BF16),
        in_specs=[anywhere, inside, anywhere, anywhere, anywhere, inside, anywhere, inside, anywhere, anywhere, anywhere]
        + [inside] * 5,
        out_specs=anywhere,
        scratch_shapes=[
            pltpu.VMEM((D, 2048), BF16),
            pltpu.VMEM((D, 1024), BF16),
            pltpu.VMEM((D, 2 * UNITS), BF16),
            pltpu.VMEM((D, UNITS), BF16),
            pltpu.VMEM((LEN, D), BF16),
            pltpu.VMEM((LEN, D), BF16),
            pltpu.VMEM((LEN, 2048), BF16),
            pltpu.VMEM((LEN, 1024), BF16),
            pltpu.VMEM((2, DK, DV), F32),
            pltpu.VMEM((LEN, UNITS), BF16),
        ]
        + [pltpu.VMEM((HALF, D), BF16)] * 3
        + [pltpu.VMEM((8, HALF, 256), BF16)] * 3
        + [
            pltpu.SemaphoreType.DMA((len(ARRAYS) * PIECES * len(OFFSETS),)),
            pltpu.SemaphoreType.DMA((len(ARRAYS),)),
            pltpu.SemaphoreType.DMA((len(ARRAYS) + 1,)),
            pltpu.SemaphoreType.DMA((11,)),
            pltpu.SemaphoreType.DMA((11,)),
            pltpu.SemaphoreType.DMA((8,)),
        ],
        compiler_params=pltpu.CompilerParams(
            collective_id=0, has_side_effects=True, vmem_limit_bytes=67043328
        ),
    )(
        resid, mix_gain.reshape(1, -1), query_weight, key_weight, value_weight, head_gain.reshape(1, -1),
        out_weight.T, mlp_gain.reshape(1, -1), gate_weight, up_weight, down_weight.T, *tables(),
    )


def solution(mesh):
    torus = Mesh(
        mesh.devices.reshape(mesh.shape["rep"], 2, 4, 4, mesh.shape["tp"]),
        ("rep", "fs_0", "fs_1", "fs_2", "tp"),
    )
    return jax.shard_map(
        shards,
        mesh=torus,
        in_specs=(
            P(REP_FS_TP, None),
            P(),
            P(FS, "tp"),
            P(FS, "tp"),
            P(FS, "tp"),
            P("tp"),
            P("tp", FS),
            P(),
            P(FS, "tp"),
            P(FS, "tp"),
            P("tp", FS),
        ),
        out_specs=P(REP_FS_TP, None),
        check_vma=False,
    )
```

```python
import heapq

import jax
import jax.numpy as jnp
import numpy as np
from jax import lax
from jax.experimental import pallas as pl
from jax.experimental.pallas import tpu as pltpu
from jax.sharding import Mesh
from jax.sharding import PartitionSpec as P

D = 2048
DK = 256
DV = 512
BLOCK = 128
LEN = 768
HALF = LEN // 2
UNITS = 1408
FS = ("fs_0", "fs_1", "fs_2")
REP_FS_TP = ("rep", "fs_0", "fs_1", "fs_2", "tp")
MESH_ID = pl.DeviceIdType.MESH
PIECES = 4
ROWS = 64
PIECE_ROWS = ROWS // PIECES
SIDE = 640
TILE = 128
ARRAYS = ((0, 0, 1024), (0, 1024, 1024), (1, 0, 1024), (2, 0, 2 * SIDE + TILE), (3, 0, SIDE + TILE))
WIDTHS = tuple(width for _, _, width in ARRAYS)
LAST = len(ARRAYS) - 1
SPLIT = (3, 4)
OFFSETS = [(z, y, x) for z in range(2) for y in range(4) for x in range(4)]
GROUPS = [(z, y) for y in (0, 1, 3, 2) for z in range(2)]
ROOT = (0, 0, 0)
F32 = jnp.float32
BF16 = jnp.bfloat16

norm_eps = 1e-06
rope_base = 10000.0


def parent(array, piece, offset):
    z, y, x = offset
    if array in SPLIT:
        if y == x == 0:
            return (4 + piece // 2, ROOT) if z else None
        if y and (piece < 2 or not x):
            up = y == 1 or (y == 2 and (x % 2 == 0 if piece < 2 else piece == 2))
            return (2, (z, y - 1, x)) if up else (3, (z, (y + 1) % 4, x))
        up = x == 1 or (x == 2 and (y % 2 == 0 if piece >= 2 else piece == 0))
        return (0, (z, y, x - 1)) if up else (1, (z, y, (x + 1) % 4))
    for axis in ("zxy", "zyx", "xzy", "yzx")[piece]:
        if axis == "z" and z:
            return 4 + (x + y + piece) % 2, (0, y, x)
        if axis == "x" and x:
            up = x == 1 or (x == 2 and (piece == 1 or (piece in (0, 2) and (y + z + piece // 2) % 2 == 0)))
            return (0, (z, y, x - 1)) if up else (1, (z, y, (x + 1) % 4))
        if axis == "y" and y:
            up = y == 1 or (y == 2 and (piece == 0 or (piece in (1, 3) and (x + z) % 2 == 0)))
            return (2, (z, y - 1, x)) if up else (3, (z, (y + 1) % 4, x))
    return None


def compute_steps():
    steps = [("prep", (), (), 2.0, None), ("norm", (0,), (), 4.0, None), ("norm", (1,), (), 4.0, None)]
    steps += [("proj", (j,), (0 if j < 4 else 1,), 1.2, None) for j in range(8)]
    steps += [("ret", (t, h), (), 0.6, None) for t in range(LEN // BLOCK) for h in range(2)]
    steps += [("out", (1, j), (2,), 0.6, None) for j in range(8)]
    steps += [("out", (0, j), (), 0.6, None) for j in range(8)]
    steps += [("mid", (r,), (), 1.5, None) for r in range(3)]
    steps += [("trade", (), (), 0.5, None)]
    steps += [("mlp", (0, i), (3,), 1.6, None) for i in range(2)]
    steps += [("mlp", (1, i), (), 1.6, None) for i in range(2)]
    steps += [("pass", (i,), (), 0.3, (("mid", (i,)), 14.0 + 3.0 * i)) for i in range(3)]
    steps += [("mlp", (2, i), (), 1.6, None) for i in range(2)]
    steps += [("mlp", (3, i), (), 1.6, None) for i in range(2)]
    steps += [("down", (g,), (("g", g),), 2.4, None) for g in range(8)]
    return steps


def program_order(steps, rate=47.0e3, latency=2.2, lead=8.0, spare=2.5):
    kids = {}
    for array in range(len(WIDTHS)):
        for piece in range(PIECES):
            for offset in OFFSETS[1:]:
                d, above = parent(array, piece, offset)
                kids.setdefault((array, piece, above), []).append((offset, d))

    def depth(*at):
        return max([0] + [1 + depth(*at[:2], c) for c, _ in kids.get(at, [])])

    def rank(array, piece, child):
        if array == LAST:
            return (array, max(GROUPS.index(child[:2]), 0), -depth(array, piece, child))
        return (array, 0, -depth(array, piece, child))

    def needs(dep):
        if isinstance(dep, tuple):
            return [(LAST, p, o) for p in range(PIECES) for o in OFFSETS if o[:2] == GROUPS[dep[1]]]
        return [(dep, p, o) for p in range(PIECES) for o in OFFSETS]

    ready = [[] for _ in range(6)]
    free = [0.0] * 6
    coming, arrival = [], {}
    for array in range(len(WIDTHS)):
        for piece in range(PIECES):
            heapq.heappush(coming, (8.0 if array in SPLIT else 2.0, (array, piece, ROOT)))
    left = [PIECES * len(OFFSETS)] * len(WIDTHS)
    order, now, todo, done = [], 0.0, list(steps), {}

    def room(d):
        early = ready[d][0][0][0] <= min(a for a in range(len(WIDTHS)) if left[a])
        return lead if early else spare

    while todo or coming or any(ready):
        while coming and coming[0][0] <= now + 1e-9:
            at, item = heapq.heappop(coming)
            arrival[item] = at
            array, piece, offset = item
            left[array] -= 1
            for child, d in kids.get(item, []):
                heapq.heappush(ready[d], (rank(array, piece, child), piece, child, offset))
        issued = False
        for d in range(6):
            while ready[d] and free[d] - now < room(d):
                (array, *_), piece, child, offset = heapq.heappop(ready[d])
                free[d] = max(free[d], now) + WIDTHS[array] * 2 * PIECE_ROWS / rate
                heapq.heappush(coming, (free[d] + latency, (array, piece, child)))
                order.append(("send", now, (d, array, piece, offset, child)))
                now += 0.03
                issued = True
        if issued:
            continue
        if todo:
            name, args, deps, cost, after = todo[0]
            start = done[after[0]] + after[1] if after else 0.0
            wanted = [c for dep in deps for c in needs(dep)]
            if now >= start and all(c in arrival for c in wanted):
                wanted.sort(key=lambda c: (arrival[c], c))
                order.append((name, now, (args, wanted)))
                now += cost
                done[name, args] = now
                todo.pop(0)
                continue
        nexts = [free[d] - room(d) + 1e-3 for d in range(6) if ready[d]]
        if coming:
            nexts.append(coming[0][0])
        if todo and start > now:
            nexts.append(start)
        now = max(now, min(nexts))
    return order, arrival, now, max(free)


STEPS = compute_steps()
ORDER, ARRIVAL, _, _ = program_order(STEPS)


def tables():
    position = np.arange(LEN, dtype=np.float32)
    inverse = np.float32(1.0) / np.float32(rope_base) ** np.linspace(0.0, 1.0, DK // 2, dtype=np.float32)
    angle = position[:, None] * inverse[None, :]
    log_gamma = np.log1p(-(2.0 ** (-5.0 - 2.0 * np.arange(4))))
    offset = np.arange(BLOCK)
    distance = offset[:, None] - offset[None, :]
    inside = np.where(distance >= 0, np.exp(log_gamma[:, None, None] * np.maximum(distance, 0)), 0.0)
    query_decay = np.exp(log_gamma[:, None] * (offset + 1.0))
    key_decay = np.exp(log_gamma[:, None] * (BLOCK - 1.0 - offset))
    wide = np.ones((1, 1, BLOCK))
    found = (np.cos(angle), np.sin(angle), inside, query_decay[:, :, None] * wide, key_decay[:, :, None] * wide)
    return tuple(jnp.asarray(t.astype(np.float32)) for t in found)


def layer_kernel(
    resid, mix_gain, q_ref, k_ref, v_ref, head_gain, o_ref, mlp_gain, g_ref, u_ref, d_ref,
    cosine, sine, inside, query_decay, key_decay,
    result,
    wq, wo, wm, wd, other_m, other_d, mixed, rows_in, normed, foreign, proj, heads, state, hidden,
    keep, give, take, keep2, give2, take2, sums, back,
    recv, send, local, swap_send, swap_recv, put,
):
    buffers = (wq, wo, wm, wd)
    rep, lo, my, mx, core = (lax.axis_index(a) for a in REP_FS_TP)
    z = rep * 2 + lo
    zu, zd = lax.rem(z + 1, 4), lax.rem(z + 3, 4)
    peers = (
        {"fs_2": lax.rem(mx + 1, 4)},
        {"fs_2": lax.rem(mx + 3, 4)},
        {"fs_1": lax.rem(my + 1, 4)},
        {"fs_1": lax.rem(my + 3, 4)},
        {"rep": zu // 2, "fs_0": lax.rem(zu, 2)},
        {"rep": zd // 2, "fs_0": lax.rem(zd, 2)},
    )
    partner = {"tp": 1 - core}
    barrier = pltpu.get_barrier_semaphore()
    for peer in peers + (partner,):
        pl.semaphore_signal(barrier, inc=1, device_id=peer, device_id_type=MESH_ID)

    def base(offset):
        oz, oy, ox = offset
        owner = (lax.rem(lo + oz, 2) * 4 + lax.rem(my + 4 - oy, 4)) * 4 + lax.rem(mx + 4 - ox, 4)
        return owner * ROWS

    own = pl.ds(pl.multiple_of(base(ROOT), ROWS), ROWS)
    mine = pl.multiple_of(core * HALF, HALF)
    other = pl.multiple_of(HALF - core * HALF, HALF)
    half = (mine, other)

    ze, zb = lax.rem(z + 1 + 2 * core, 4), lax.rem(z + 3 - 2 * core, 4)
    helper = {"rep": ze // 2, "fs_0": lax.rem(ze, 2)}
    helped = {"rep": zb // 2, "fs_0": lax.rem(zb, 2)}

    here_m = pl.ds(pl.multiple_of(lo * (SIDE + TILE), TILE), SIDE)
    here_d = pl.ds(pl.multiple_of((1 - lo) * (SIDE + TILE), TILE), SIDE)
    tile = pl.ds(SIDE, TILE)
    left, right = pl.ds(0, SIDE), pl.ds(SIDE + TILE, SIDE)
    parts = {
        0: [(q_ref, wq.at[own, pl.ds(0, 512)]), (k_ref, wq.at[own, pl.ds(512, 512)])],
        1: [(v_ref, wq.at[own, pl.ds(1024, 1024)])],
        2: [(o_ref, wo.at[own, :])],
        3: [
            (g_ref.at[:, tile], mixed.at[0]),
            (u_ref.at[:, tile], mixed.at[1]),
            (g_ref.at[:, here_m], wm.at[own, left]),
            (u_ref.at[:, here_m], wm.at[own, right]),
            (g_ref.at[:, here_d], other_m.at[:, left]),
            (u_ref.at[:, here_d], other_m.at[:, right]),
        ],
        4: [
            (d_ref.at[:, here_m], wd.at[own, left]),
            (d_ref.at[:, tile], wd.at[own, tile]),
            (d_ref.at[:, here_d], other_d.at[:, left]),
            (d_ref.at[:, tile], other_d.at[:, tile]),
        ],
    }
    fills = {}
    for array, pairs in parts.items():
        fills[array] = []
        for source, there in pairs:
            at = sum(len(f) for f in fills.values())
            fills[array].append(pltpu.make_async_copy(source, there, local.at[at]))
            fills[array][-1].start()
    fill = pltpu.make_async_copy(resid, rows_in.at[pl.ds(mine, HALF), :], local.at[15])
    fill.start()
    pl.semaphore_wait(barrier, 7)

    def swap(source, there, slot, device=partner):
        return pltpu.make_async_remote_copy(
            src_ref=source,
            dst_ref=there,
            send_sem=swap_send.at[slot],
            recv_sem=swap_recv.at[slot],
            device_id=device,
            device_id_type=MESH_ID,
        )

    swaps = {0: swap(resid, rows_in.at[pl.ds(mine, HALF), :], 0)}
    swaps[0].start()

    def chunk(array, piece, offset):
        buffer, first, width = ARRAYS[array]
        start = pl.multiple_of(base(offset) + piece * PIECE_ROWS, PIECE_ROWS)
        return buffers[buffer].at[pl.ds(start, PIECE_ROWS), pl.ds(first, width)]

    def slot_of(array, piece, offset):
        return (array * PIECES + piece) * len(OFFSETS) + OFFSETS.index(offset)

    waited = set()

    def arrive(array, piece, offset):
        key = (array,) if offset == ROOT else (array, piece, offset)
        if key in waited:
            return
        waited.add(key)
        if offset == ROOT:
            for item in fills[array]:
                item.wait()
        else:
            here = chunk(array, piece, offset)
            pltpu.make_async_copy(here, here, recv.at[slot_of(array, piece, offset)]).wait()

    def prepare():
        arrive(3, 0, ROOT)
        lane = lax.broadcasted_iota(jnp.int32, (ROWS, TILE), 1) // (TILE // 2)
        gate = mixed[0].astype(F32)
        up = pltpu.roll(mixed[1].astype(F32), TILE // 2, 1)
        wm[own, tile] = jnp.where(lane == lo, gate, up).astype(BF16)
        other_m[:, tile] = jnp.where(lane == 1 - lo, gate, up).astype(BF16)

    def norm_rows(source, gain, start, count):
        def some(i, _):
            rows = pl.ds(pl.multiple_of(start + i * 32, 32), 32)
            wide = source[rows, :].astype(F32)
            scaled = wide * lax.rsqrt(jnp.mean(wide * wide, axis=-1, keepdims=True) + norm_eps)
            normed[rows, :] = (scaled * gain[...]).astype(BF16)

        lax.fori_loop(0, count // 32, some, None)

    def norm(which):
        if which == 0:
            fill.wait()
        else:
            swaps[0].wait()
        norm_rows(rows_in, mix_gain, half[which], HALF)

    def project(j):
        def some(i, _):
            rows = pl.ds(pl.multiple_of(i * HALF, HALF), HALF)
            columns = pl.ds(256 * j, 256)
            found = jnp.dot(normed[rows, :], wq[:, columns], preferred_element_type=F32).astype(BF16)
            if j < 4:
                wide = found.astype(F32)
                first, second = wide[:, :128], wide[:, 128:]
                c, s = cosine[rows, :], sine[rows, :]
                turned = jnp.concatenate([first * c - second * s, second * c + first * s], axis=1)
                if j >= 2:
                    turned = turned * DK**-0.5
                found = turned.astype(BF16)
            proj[rows, columns] = found

        lax.fori_loop(0, 2, some, None)

    def retain(t, h):
        rows = pl.ds(t * BLOCK, BLOCK)
        head = core * 2 + h
        queries = proj[rows, pl.ds(DK * h, DK)]
        keys = proj[rows, pl.ds(2 * DK + DK * h, DK)]
        values = proj[rows, pl.ds(4 * DK + DV * h, DV)]
        decay = query_decay[head]
        scores = lax.dot_general(queries, keys, (((1,), (1,)), ((), ())), preferred_element_type=F32)
        weights = (scores * inside[head]).astype(BF16)
        found = jnp.dot(weights, values, preferred_element_type=F32)
        if t > 0:
            carried = jnp.dot(queries, state[h].astype(BF16), preferred_element_type=F32)
            found = found + carried * jnp.concatenate([decay] * 4, axis=1)
        if t < LEN // BLOCK - 1:
            fade = key_decay[head]
            faded = (keys.astype(F32) * jnp.concatenate([fade] * 2, axis=1)).astype(BF16)
            fresh = lax.dot_general(faded, values, (((0,), (0,)), ((), ())), preferred_element_type=F32)
            if t > 0:
                last = query_decay[head, BLOCK - 1 : BLOCK, :]
                fresh = state[h] * jnp.concatenate([last] * 4, axis=1) + fresh
            state[h] = fresh
        columns = pl.ds(DV * h, DV)
        scaled = found * lax.rsqrt(jnp.mean(found * found, axis=-1, keepdims=True) + norm_eps)
        heads[rows, columns] = (scaled * head_gain[:, columns]).astype(BF16)

    def give_heads(which, j):
        columns = pl.ds(256 * j, 256)
        share = lax.dot_general(
            heads[pl.ds(half[which], HALF), :], wo[columns, :], (((1,), (1,)), ((), ())), preferred_element_type=F32
        ).astype(BF16)
        (give if which else keep)[:, columns] = share
        if (which, j) == (0, 0):
            swaps[1] = swap(give, take, 1)
            swaps[1].start()

    third = HALF // 3

    def lend(r):
        here = normed.at[pl.ds(pl.multiple_of(mine + r * third, third), third), :]
        swaps[2 + r] = swap(here, foreign.at[core, pl.ds(r * third, third), :], 2 + r, helper)
        swaps[5 + r] = swap(here, here, 5 + r)
        swaps[2 + r].start()
        swaps[5 + r].start()

    def middle(r):
        if r == 0:
            swaps[1].wait()

        def some(i, _):
            here = pl.ds(pl.multiple_of(r * third + i * 32, 32), 32)
            rows = pl.ds(pl.multiple_of(mine + r * third + i * 32, 32), 32)
            added = keep[here, :].astype(F32) + take[here, :].astype(F32)
            found = (rows_in[rows, :].astype(F32) + added).astype(BF16)
            rows_in[rows, :] = found
            wide = found.astype(F32)
            scaled = wide * lax.rsqrt(jnp.mean(wide * wide, axis=-1, keepdims=True) + norm_eps)
            normed[rows, :] = (scaled * mlp_gain[...]).astype(BF16)

        lax.fori_loop(0, third // 32, some, None)
        if r > 0:
            lend(r - 1)

    def trade():
        lend(2)

    def forward(i):
        swaps[2 + i].wait()
        here = foreign.at[core, pl.ds(i * third, third), :]
        swaps[8 + i] = swap(here, here, 8 + i)
        swaps[8 + i].start()

    quarter = HALF // 2

    def expand(part, i):
        if (part, i) == (1, 0):
            for r in range(3):
                swaps[5 + r].wait()
        if (part, i) == (3, 0):
            for r in range(3):
                swaps[8 + r].wait()
        side = core if part % 2 == 0 else 1 - core
        if part < 2:
            source = normed[pl.ds(pl.multiple_of(side * HALF + i * quarter, quarter), quarter), :]
        else:
            source = foreign[side, pl.ds(i * quarter, quarter), :]
        both = jnp.dot(source, wm[...], preferred_element_type=F32)
        place = 2 * (part // 2) + side
        rows = pl.ds(i * quarter, quarter)
        hidden[place, rows, pl.ds(0, SIDE)] = (
            jax.nn.silu(both[:, :SIDE]) * both[:, SIDE + TILE :]
        ).astype(BF16)
        shared = both[:, SIDE : SIDE + TILE]
        found = jax.nn.silu(shared) * pltpu.roll(shared, TILE // 2, 1)
        lane = lax.broadcasted_iota(jnp.int32, (quarter, TILE), 1) // (TILE // 2)
        hidden[place, rows, tile] = jnp.where(lane == lo, found, 0.0).astype(BF16)

    blocks = {}

    def contract(g):
        oz, oy = GROUPS[g]
        block = lax.rem(lo + oz, 2) * 4 + lax.rem(my + 4 - oy, 4)
        blocks[g] = block
        weights = wd.at[pl.ds(pl.multiple_of(block * 256, 256), 256), :]

        def some(i, _):
            for kept, side in ((give2, 1 - core), (keep2, core)):
                kept[block, i] = lax.dot_general(
                    hidden[2 * i + side], weights[...], (((1,), (1,)), ((), ())), preferred_element_type=F32
                ).astype(BF16)

        lax.fori_loop(0, 2, some, None)
        swaps[11 + g] = swap(give2.at[block], take2.at[block], 11 + g)
        swaps[11 + g].start()

    def add_foreign(g):
        swaps[11 + g].wait()
        block = blocks[g]

        def some(i, _):
            rows = pl.ds(pl.multiple_of(i * 96, 32), 96)
            added = keep2[block, 1, rows, :].astype(F32) + take2[block, 1, rows, :].astype(F32)
            sums[block, rows, :] = added.astype(BF16)

        lax.fori_loop(0, HALF // 96, some, None)

    def send_back(g):
        swaps[19 + g] = swap(sums.at[blocks[g]], back.at[blocks[g]], 19 + g, helped)
        swaps[19 + g].start()

    def writing(g):
        place = result.at[:, pl.ds(pl.multiple_of(blocks[g] * 256, 256), 256)]
        return pltpu.make_async_copy(keep2.at[blocks[g], 0], place, put.at[g])

    def finish(g):
        block = blocks[g]
        swaps[19 + g].wait_send()
        swap(sums.at[block], back.at[block], 19 + (g ^ 1), helped).wait_recv()

        def some(i, _):
            here = pl.ds(pl.multiple_of(i * 96, 32), 96)
            rows = pl.ds(pl.multiple_of(mine + i * 96, 32), 96)
            columns = pl.ds(pl.multiple_of(block * 256, 256), 256)
            added = keep2[block, 0, here, :].astype(F32) + take2[block, 0, here, :].astype(F32)
            added = added + back[block, here, :].astype(F32)
            keep2[block, 0, here, :] = (rows_in[rows, columns].astype(F32) + added).astype(BF16)

        lax.fori_loop(0, HALF // 96, some, None)
        writing(g).start()

    def after_down(g):
        if 0 <= g - 1 < len(GROUPS):
            add_foreign(g - 1)
        if 0 <= g - 4 < len(GROUPS):
            finish(g - 4)
        if 0 <= g - 1 < len(GROUPS):
            send_back(g - 1)

    def down(g):
        contract(g)
        after_down(g)

    run = {
        "prep": prepare, "norm": norm, "proj": project, "ret": retain, "out": give_heads,
        "mid": middle, "trade": trade, "pass": forward, "mlp": expand, "down": down,
    }
    for name, _, what in ORDER:
        if name == "send":
            d, array, piece, offset, child = what
            arrive(array, piece, offset)
            source = here = chunk(array, piece, offset)
            if array in SPLIT and child == (1, 0, 0):
                source = (other_m, other_d)[array - 3].at[pl.ds(piece * PIECE_ROWS, PIECE_ROWS), :]
            pltpu.make_async_remote_copy(
                src_ref=source,
                dst_ref=here,
                send_sem=send.at[array],
                recv_sem=recv.at[slot_of(array, piece, child)],
                device_id=peers[d],
                device_id_type=MESH_ID,
            ).start()
        else:
            args, wanted = what
            for item in wanted:
                arrive(*item)
            run[name](*args)
    for g in range(len(GROUPS), len(GROUPS) + 4):
        after_down(g)
    for array, (buffer, first, width) in enumerate(ARRAYS):
        sent = buffers[buffer].at[pl.ds(0, 31 * ROWS), pl.ds(first, width)]
        pltpu.make_async_copy(sent, sent, send.at[array]).wait()
    for g in range(len(GROUPS)):
        writing(g).wait()


def shards(
    resid, mix_gain, query_weight, key_weight, value_weight, head_gain, out_weight, mlp_gain,
    gate_weight, up_weight, down_weight,
):
    anywhere = pl.BlockSpec(memory_space=pl.ANY)
    inside = pl.BlockSpec(memory_space=pltpu.VMEM)
    return pl.pallas_call(
        layer_kernel,
        out_shape=jax.ShapeDtypeStruct((HALF, D), BF16),
        in_specs=[anywhere, inside, anywhere, anywhere, anywhere, inside, anywhere, inside, anywhere, anywhere, anywhere]
        + [inside] * 5,
        out_specs=anywhere,
        scratch_shapes=[
            pltpu.VMEM((D, 2048), BF16),
            pltpu.VMEM((D, 1024), BF16),
            pltpu.VMEM((D, ARRAYS[3][2]), BF16),
            pltpu.VMEM((D, ARRAYS[4][2]), BF16),
            pltpu.VMEM((ROWS, ARRAYS[3][2]), BF16),
            pltpu.VMEM((ROWS, ARRAYS[4][2]), BF16),
            pltpu.VMEM((2, ROWS, TILE), BF16),
            pltpu.VMEM((LEN, D), BF16),
            pltpu.VMEM((LEN, D), BF16),
            pltpu.VMEM((2, HALF, D), BF16),
            pltpu.VMEM((LEN, 2048), BF16),
            pltpu.VMEM((LEN, 1024), BF16),
            pltpu.VMEM((2, DK, DV), F32),
            pltpu.VMEM((4, HALF, SIDE + TILE), BF16),
        ]
        + [pltpu.VMEM((HALF, D), BF16)] * 3
        + [pltpu.VMEM((8, 2, HALF, 256), BF16)] * 3
        + [pltpu.VMEM((8, HALF, 256), BF16)] * 2
        + [
            pltpu.SemaphoreType.DMA((len(ARRAYS) * PIECES * len(OFFSETS),)),
            pltpu.SemaphoreType.DMA((len(ARRAYS),)),
            pltpu.SemaphoreType.DMA((16,)),
            pltpu.SemaphoreType.DMA((27,)),
            pltpu.SemaphoreType.DMA((27,)),
            pltpu.SemaphoreType.DMA((8,)),
        ],
        compiler_params=pltpu.CompilerParams(
            collective_id=0, has_side_effects=True, vmem_limit_bytes=67043328
        ),
    )(
        resid, mix_gain.reshape(1, -1), query_weight, key_weight, value_weight, head_gain.reshape(1, -1),
        out_weight.T, mlp_gain.reshape(1, -1), gate_weight, up_weight, down_weight.T, *tables(),
    )


def solution(mesh):
    torus = Mesh(
        mesh.devices.reshape(mesh.shape["rep"], 2, 4, 4, mesh.shape["tp"]),
        ("rep", "fs_0", "fs_1", "fs_2", "tp"),
    )
    return jax.shard_map(
        shards,
        mesh=torus,
        in_specs=(
            P(REP_FS_TP, None),
            P(),
            P(FS, "tp"),
            P(FS, "tp"),
            P(FS, "tp"),
            P("tp"),
            P("tp", FS),
            P(),
            P(FS, "tp"),
            P(FS, "tp"),
            P("tp", FS),
        ),
        out_specs=P(REP_FS_TP, None),
        check_vma=False,
    )
```

```python
import heapq

import jax
import jax.numpy as jnp
import numpy as np
from jax import lax
from jax.experimental import pallas as pl
from jax.experimental.pallas import tpu as pltpu
from jax.sharding import Mesh
from jax.sharding import PartitionSpec as P

D = 2048
DK = 256
DV = 512
BLOCK = 128
LEN = 768
HALF = LEN // 2
UNITS = 1408
FS = ("fs_0", "fs_1", "fs_2")
REP_FS_TP = ("rep", "fs_0", "fs_1", "fs_2", "tp")
MESH_ID = pl.DeviceIdType.MESH
PIECES = 4
ROWS = 64
PIECE_ROWS = ROWS // PIECES
SIDE = 640
TILE = 128
ARRAYS = ((0, 0, 1024), (0, 1024, 1024), (1, 0, 1024), (2, 0, 2 * SIDE + TILE), (3, 0, SIDE + TILE))
WIDTHS = tuple(width for _, _, width in ARRAYS)
LAST = len(ARRAYS) - 1
SPLIT = (3, 4)
DUE = (20, 25, 30, 78, 86)
HOP = 4.0
LEAD = 4.0
OFFSETS = [(z, y, x) for z in range(2) for y in range(4) for x in range(4)]
GROUPS = [(z, y) for y in (0, 1, 3, 2) for z in range(2)]
ROOT = (0, 0, 0)
F32 = jnp.float32
BF16 = jnp.bfloat16

norm_eps = 1e-06
rope_base = 10000.0


def parent(array, piece, offset):
    z, y, x = offset
    if array in SPLIT:
        if y == x == 0:
            return (4 + piece // 2, ROOT) if z else None
        if y and (piece < 2 or not x):
            up = y == 1 or (y == 2 and (x % 2 == 0 if piece < 2 else piece == 2))
            return (2, (z, y - 1, x)) if up else (3, (z, (y + 1) % 4, x))
        up = x == 1 or (x == 2 and (y % 2 == 0 if piece >= 2 else piece == 0))
        return (0, (z, y, x - 1)) if up else (1, (z, y, (x + 1) % 4))
    for axis in ("zxy", "zyx", "xzy", "yzx")[piece]:
        if axis == "z" and z:
            return 4 + (x + y + piece) % 2, (0, y, x)
        if axis == "x" and x:
            up = x == 1 or (x == 2 and (piece == 1 or (piece in (0, 2) and (y + z + piece // 2) % 2 == 0)))
            return (0, (z, y, x - 1)) if up else (1, (z, y, (x + 1) % 4))
        if axis == "y" and y:
            up = y == 1 or (y == 2 and (piece == 0 or (piece in (1, 3) and (x + z) % 2 == 0)))
            return (2, (z, y - 1, x)) if up else (3, (z, (y + 1) % 4, x))
    return None


def compute_steps():
    steps = [("prep", (), (), 2.0, None), ("norm", (0,), (), 4.0, None), ("norm", (1,), (), 4.0, None)]
    steps += [("proj", (j,), (0 if j < 4 else 1,), 1.2, None) for j in range(8)]
    steps += [("ret", (t, h), (), 0.6, None) for t in range(LEN // BLOCK) for h in range(2)]
    for r in range(3):
        steps += [("out", (1, r), (2,), 1.2, None), ("out", (0, r), (), 1.2, None), ("mid", (r,), (), 1.0, None)]
    steps += [("pass", (i,), (), 0.1, (("mid", (i,)), 8.5 + 3.0 * i)) for i in range(3)]
    steps += [("mlp", (2, i), (3,), 1.6, None) for i in range(2)]
    steps += [("mlp", (3, i), (), 1.6, None) for i in range(2)]
    tail = [("mlp", (0, i), (), 1.6, None) for i in range(2)] + [("mlp", (1, i), (), 1.6, None) for i in range(2)]
    tail += [("own", (g,), (), 1.0, None) for g in range(8)]
    for g in range(8):
        steps += [("lent", (g,), (("g", g),), 1.2, None)] + (tail[g // 2 : g // 2 + 1] if g % 2 else [])
    return steps + tail[4:]


def program_order(steps, rate=47.0e3, latency=2.2, lead=LEAD):
    kids = {}
    for array in range(len(WIDTHS)):
        for piece in range(PIECES):
            for offset in OFFSETS[1:]:
                d, above = parent(array, piece, offset)
                kids.setdefault((array, piece, above), []).append((offset, d))

    def depth(*at):
        return max([0] + [1 + depth(*at[:2], c) for c, _ in kids.get(at, [])])

    def due(array, piece, child):
        late = GROUPS.index(child[:2]) if array == LAST else 0
        return DUE[array] + late - HOP * depth(array, piece, child)

    def needs(dep):
        if isinstance(dep, tuple):
            return [(LAST, p, o) for p in range(PIECES) for o in OFFSETS if o[:2] == GROUPS[dep[1]]]
        return [(dep, p, o) for p in range(PIECES) for o in OFFSETS]

    ready = [[] for _ in range(6)]
    free = [0.0] * 6
    coming, arrival = [], {}
    for array in range(len(WIDTHS)):
        for piece in range(PIECES):
            heapq.heappush(coming, (8.0 if array in SPLIT else 2.0, (array, piece, ROOT)))
    order, now, todo, done = [], 0.0, list(steps), {}

    while todo or coming or any(ready):
        while coming and coming[0][0] <= now + 1e-9:
            at, item = heapq.heappop(coming)
            arrival[item] = at
            array, piece, offset = item
            for child, d in kids.get(item, []):
                heapq.heappush(ready[d], (due(array, piece, child), array, piece, child, offset))
        issued = False
        for d in range(6):
            while ready[d] and free[d] - now < lead:
                _, array, piece, child, offset = heapq.heappop(ready[d])
                free[d] = max(free[d], now) + WIDTHS[array] * 2 * PIECE_ROWS / rate
                heapq.heappush(coming, (free[d] + latency, (array, piece, child)))
                order.append(("send", now, (d, array, piece, offset, child)))
                now += 0.03
                issued = True
        if issued:
            continue
        if todo:
            name, args, deps, cost, after = todo[0]
            start = done[after[0]] + after[1] if after else 0.0
            wanted = [c for dep in deps for c in needs(dep)]
            if now >= start and all(c in arrival for c in wanted):
                wanted.sort(key=lambda c: (arrival[c], c))
                order.append((name, now, (args, wanted)))
                now += cost
                done[name, args] = now
                todo.pop(0)
                continue
        nexts = [free[d] - lead + 1e-3 for d in range(6) if ready[d]]
        if coming:
            nexts.append(coming[0][0])
        if todo and start > now:
            nexts.append(start)
        now = max(now, min(nexts))
    return order, arrival, now, max(free)


STEPS = compute_steps()
ORDER, ARRIVAL, _, _ = program_order(STEPS)


def tables():
    position = np.arange(LEN, dtype=np.float32)
    inverse = np.float32(1.0) / np.float32(rope_base) ** np.linspace(0.0, 1.0, DK // 2, dtype=np.float32)
    angle = position[:, None] * inverse[None, :]
    log_gamma = np.log1p(-(2.0 ** (-5.0 - 2.0 * np.arange(4))))
    offset = np.arange(BLOCK)
    distance = offset[:, None] - offset[None, :]
    inside = np.where(distance >= 0, np.exp(log_gamma[:, None, None] * np.maximum(distance, 0)), 0.0)
    query_decay = np.exp(log_gamma[:, None] * (offset + 1.0))
    key_decay = np.exp(log_gamma[:, None] * (BLOCK - 1.0 - offset))
    wide = np.ones((1, 1, BLOCK))
    found = (np.cos(angle), np.sin(angle), inside, query_decay[:, :, None] * wide, key_decay[:, :, None] * wide)
    return tuple(jnp.asarray(t.astype(np.float32)) for t in found)


def layer_kernel(
    resid, mix_gain, q_ref, k_ref, v_ref, head_gain, o_ref, mlp_gain, g_ref, u_ref, d_ref,
    cosine, sine, inside, query_decay, key_decay,
    result,
    wq, wo, wm, wd, other_m, other_d, mixed, rows_in, normed, foreign, proj, heads, state, hidden,
    keep, give, take, both2, take2, sums, back,
    recv, send, local, swap_send, swap_recv, put,
):
    buffers = (wq, wo, wm, wd)
    rep, lo, my, mx, core = (lax.axis_index(a) for a in REP_FS_TP)
    z = rep * 2 + lo
    zu, zd = lax.rem(z + 1, 4), lax.rem(z + 3, 4)
    peers = (
        {"fs_2": lax.rem(mx + 1, 4)},
        {"fs_2": lax.rem(mx + 3, 4)},
        {"fs_1": lax.rem(my + 1, 4)},
        {"fs_1": lax.rem(my + 3, 4)},
        {"rep": zu // 2, "fs_0": lax.rem(zu, 2)},
        {"rep": zd // 2, "fs_0": lax.rem(zd, 2)},
    )
    partner = {"tp": 1 - core}
    barrier = pltpu.get_barrier_semaphore()
    for peer in peers + (partner,):
        pl.semaphore_signal(barrier, inc=1, device_id=peer, device_id_type=MESH_ID)

    def base(offset):
        oz, oy, ox = offset
        owner = (lax.rem(lo + oz, 2) * 4 + lax.rem(my + 4 - oy, 4)) * 4 + lax.rem(mx + 4 - ox, 4)
        return owner * ROWS

    own = pl.ds(pl.multiple_of(base(ROOT), ROWS), ROWS)
    mine = pl.multiple_of(core * HALF, HALF)
    other = pl.multiple_of(HALF - core * HALF, HALF)
    half = (mine, other)

    ze, zb = lax.rem(z + 1 + 2 * core, 4), lax.rem(z + 3 - 2 * core, 4)
    helper = {"rep": ze // 2, "fs_0": lax.rem(ze, 2)}
    helped = {"rep": zb // 2, "fs_0": lax.rem(zb, 2)}

    here_m = pl.ds(pl.multiple_of(lo * (SIDE + TILE), TILE), SIDE)
    here_d = pl.ds(pl.multiple_of((1 - lo) * (SIDE + TILE), TILE), SIDE)
    tile = pl.ds(SIDE, TILE)
    left, right = pl.ds(0, SIDE), pl.ds(SIDE + TILE, SIDE)
    parts = {
        0: [(q_ref, wq.at[own, pl.ds(0, 512)]), (k_ref, wq.at[own, pl.ds(512, 512)])],
        1: [(v_ref, wq.at[own, pl.ds(1024, 1024)])],
        2: [(o_ref, wo.at[own, :])],
        3: [
            (g_ref.at[:, tile], mixed.at[0]),
            (u_ref.at[:, tile], mixed.at[1]),
            (g_ref.at[:, here_m], wm.at[own, left]),
            (u_ref.at[:, here_m], wm.at[own, right]),
            (g_ref.at[:, here_d], other_m.at[:, left]),
            (u_ref.at[:, here_d], other_m.at[:, right]),
        ],
        4: [
            (d_ref.at[:, here_m], wd.at[own, left]),
            (d_ref.at[:, tile], wd.at[own, tile]),
            (d_ref.at[:, here_d], other_d.at[:, left]),
            (d_ref.at[:, tile], other_d.at[:, tile]),
        ],
    }
    fills = {}
    for array, pairs in parts.items():
        fills[array] = []
        for source, there in pairs:
            at = sum(len(f) for f in fills.values())
            fills[array].append(pltpu.make_async_copy(source, there, local.at[at]))
            fills[array][-1].start()
    fill = pltpu.make_async_copy(resid, rows_in.at[pl.ds(mine, HALF), :], local.at[15])
    fill.start()
    pl.semaphore_wait(barrier, 7)

    def swap(source, there, slot, device=partner):
        return pltpu.make_async_remote_copy(
            src_ref=source,
            dst_ref=there,
            send_sem=swap_send.at[slot],
            recv_sem=swap_recv.at[slot],
            device_id=device,
            device_id_type=MESH_ID,
        )

    swaps = {0: swap(resid, rows_in.at[pl.ds(mine, HALF), :], 0)}
    swaps[0].start()

    def chunk(array, piece, offset):
        buffer, first, width = ARRAYS[array]
        start = pl.multiple_of(base(offset) + piece * PIECE_ROWS, PIECE_ROWS)
        return buffers[buffer].at[pl.ds(start, PIECE_ROWS), pl.ds(first, width)]

    def slot_of(array, piece, offset):
        return (array * PIECES + piece) * len(OFFSETS) + OFFSETS.index(offset)

    waited = set()

    def arrive(array, piece, offset):
        key = (array,) if offset == ROOT else (array, piece, offset)
        if key in waited:
            return
        waited.add(key)
        if offset == ROOT:
            for item in fills[array]:
                item.wait()
        else:
            here = chunk(array, piece, offset)
            pltpu.make_async_copy(here, here, recv.at[slot_of(array, piece, offset)]).wait()

    def prepare():
        arrive(3, 0, ROOT)
        lane = lax.broadcasted_iota(jnp.int32, (ROWS, TILE), 1) // (TILE // 2)
        gate = mixed[0].astype(F32)
        up = pltpu.roll(mixed[1].astype(F32), TILE // 2, 1)
        wm[own, tile] = jnp.where(lane == lo, gate, up).astype(BF16)
        other_m[:, tile] = jnp.where(lane == 1 - lo, gate, up).astype(BF16)

    def norm_rows(source, gain, start, count):
        def some(i, _):
            rows = pl.ds(pl.multiple_of(start + i * 32, 32), 32)
            wide = source[rows, :].astype(F32)
            scaled = wide * lax.rsqrt(jnp.mean(wide * wide, axis=-1, keepdims=True) + norm_eps)
            normed[rows, :] = (scaled * gain[...]).astype(BF16)

        lax.fori_loop(0, count // 32, some, None)

    def norm(which):
        if which == 0:
            fill.wait()
        else:
            swaps[0].wait()
        norm_rows(rows_in, mix_gain, half[which], HALF)

    def project(j):
        def some(i, _):
            rows = pl.ds(pl.multiple_of(i * HALF, HALF), HALF)
            columns = pl.ds(256 * j, 256)
            found = jnp.dot(normed[rows, :], wq[:, columns], preferred_element_type=F32).astype(BF16)
            if j < 4:
                wide = found.astype(F32)
                first, second = wide[:, :128], wide[:, 128:]
                c, s = cosine[rows, :], sine[rows, :]
                turned = jnp.concatenate([first * c - second * s, second * c + first * s], axis=1)
                if j >= 2:
                    turned = turned * DK**-0.5
                found = turned.astype(BF16)
            proj[rows, columns] = found

        lax.fori_loop(0, 2, some, None)

    def retain(t, h):
        rows = pl.ds(t * BLOCK, BLOCK)
        head = core * 2 + h
        queries = proj[rows, pl.ds(DK * h, DK)]
        keys = proj[rows, pl.ds(2 * DK + DK * h, DK)]
        values = proj[rows, pl.ds(4 * DK + DV * h, DV)]
        decay = query_decay[head]
        scores = lax.dot_general(queries, keys, (((1,), (1,)), ((), ())), preferred_element_type=F32)
        weights = (scores * inside[head]).astype(BF16)
        found = jnp.dot(weights, values, preferred_element_type=F32)
        if t > 0:
            carried = jnp.dot(queries, state[h].astype(BF16), preferred_element_type=F32)
            found = found + carried * jnp.concatenate([decay] * 4, axis=1)
        if t < LEN // BLOCK - 1:
            fade = key_decay[head]
            faded = (keys.astype(F32) * jnp.concatenate([fade] * 2, axis=1)).astype(BF16)
            fresh = lax.dot_general(faded, values, (((0,), (0,)), ((), ())), preferred_element_type=F32)
            if t > 0:
                last = query_decay[head, BLOCK - 1 : BLOCK, :]
                fresh = state[h] * jnp.concatenate([last] * 4, axis=1) + fresh
            state[h] = fresh
        columns = pl.ds(DV * h, DV)
        scaled = found * lax.rsqrt(jnp.mean(found * found, axis=-1, keepdims=True) + norm_eps)
        heads[rows, columns] = (scaled * head_gain[:, columns]).astype(BF16)

    third = HALF // 3

    def give_heads(which, r):
        rows = pl.ds(pl.multiple_of(half[which] + r * third, third), third)
        there = pl.ds(r * third, third)
        share = give if which else keep

        def some(j, _):
            columns = pl.ds(pl.multiple_of(j * 512, 512), 512)
            share[there, columns] = lax.dot_general(
                heads[rows, :], wo[columns, :], (((1,), (1,)), ((), ())), preferred_element_type=F32
            ).astype(BF16)

        lax.fori_loop(0, 4, some, None)
        if which:
            swaps[35 + r] = swap(give.at[there, :], take.at[there, :], 35 + r)
            swaps[35 + r].start()

    def lend(r):
        here = normed.at[pl.ds(pl.multiple_of(mine + r * third, third), third), :]
        swaps[2 + r] = swap(here, foreign.at[core, pl.ds(r * third, third), :], 2 + r, helper)
        swaps[5 + r] = swap(here, here, 5 + r)
        swaps[2 + r].start()
        swaps[5 + r].start()

    def middle(r):
        swaps[35 + r].wait()

        def some(i, _):
            here = pl.ds(pl.multiple_of(r * third + i * 32, 32), 32)
            rows = pl.ds(pl.multiple_of(mine + r * third + i * 32, 32), 32)
            added = keep[here, :].astype(F32) + take[here, :].astype(F32)
            found = (rows_in[rows, :].astype(F32) + added).astype(BF16)
            rows_in[rows, :] = found
            wide = found.astype(F32)
            scaled = wide * lax.rsqrt(jnp.mean(wide * wide, axis=-1, keepdims=True) + norm_eps)
            normed[rows, :] = (scaled * mlp_gain[...]).astype(BF16)

        lax.fori_loop(0, third // 32, some, None)
        lend(r)

    def forward(i):
        swaps[2 + i].wait()
        here = foreign.at[core, pl.ds(i * third, third), :]
        swaps[8 + i] = swap(here, here, 8 + i)
        swaps[8 + i].start()

    quarter = HALF // 2

    def expand(part, i):
        if (part, i) == (1, 0):
            for r in range(3):
                swaps[5 + r].wait()
        if (part, i) == (3, 0):
            for r in range(3):
                swaps[8 + r].wait()
        side = core if part % 2 == 0 else 1 - core
        if part < 2:
            source = normed[pl.ds(pl.multiple_of(side * HALF + i * quarter, quarter), quarter), :]
        else:
            source = foreign[side, pl.ds(i * quarter, quarter), :]
        both = jnp.dot(source, wm[...], preferred_element_type=F32)
        place = 2 * (part // 2) + side
        rows = pl.ds(i * quarter, quarter)
        hidden[place, rows, pl.ds(0, SIDE)] = (
            jax.nn.silu(both[:, :SIDE]) * both[:, SIDE + TILE :]
        ).astype(BF16)
        shared = both[:, SIDE : SIDE + TILE]
        found = jax.nn.silu(shared) * pltpu.roll(shared, TILE // 2, 1)
        lane = lax.broadcasted_iota(jnp.int32, (quarter, TILE), 1) // (TILE // 2)
        hidden[place, rows, tile] = jnp.where(lane == lo, found, 0.0).astype(BF16)
        if part < 2:
            send_back()

    blocks = {}

    def down_into(g, part, slot):
        block = blocks[g]
        weights = wd.at[pl.ds(pl.multiple_of(block * 256, 256), 256), :]

        def some(i, _):
            side = i * core + (1 - i) * (1 - core)
            both2[block, part, i] = lax.dot_general(
                hidden[2 * part + side], weights[...], (((1,), (1,)), ((), ())), preferred_element_type=F32
            ).astype(BF16)

        lax.fori_loop(0, 2, some, None)
        swaps[slot] = swap(both2.at[block, part, 0], take2.at[block, part], slot)
        swaps[slot].start()

    pending = []

    def send_back():
        for g in pending:
            swaps[11 + g].wait()
            block = blocks[g]

            def some(i, _, block=block):
                rows = pl.ds(pl.multiple_of(i * 96, 32), 96)
                added = both2[block, 1, 1, rows, :].astype(F32) + take2[block, 1, rows, :].astype(F32)
                sums[block, rows, :] = added.astype(BF16)

            lax.fori_loop(0, HALF // 96, some, None)
            swaps[19 + g] = swap(sums.at[block], back.at[block], 19 + g, helped)
            swaps[19 + g].start()
        pending.clear()

    def lent(g):
        oz, oy = GROUPS[g]
        blocks[g] = lax.rem(lo + oz, 2) * 4 + lax.rem(my + 4 - oy, 4)
        down_into(g, 1, 11 + g)
        send_back()
        pending.append(g)

    def own_rows(g):
        down_into(g, 0, 27 + g)
        send_back()
        if g >= 2:
            finish(g - 2)

    def writing(g):
        place = result.at[:, pl.ds(pl.multiple_of(blocks[g] * 256, 256), 256)]
        return pltpu.make_async_copy(both2.at[blocks[g], 0, 1], place, put.at[g])

    def finish(g):
        block = blocks[g]
        swaps[27 + g].wait()
        swaps[19 + g].wait_send()
        swap(sums.at[block], back.at[block], 19 + (g ^ 1), helped).wait_recv()

        def some(i, _):
            here = pl.ds(pl.multiple_of(i * 96, 32), 96)
            rows = pl.ds(pl.multiple_of(mine + i * 96, 32), 96)
            columns = pl.ds(pl.multiple_of(block * 256, 256), 256)
            added = both2[block, 0, 1, here, :].astype(F32) + take2[block, 0, here, :].astype(F32)
            added = added + back[block, here, :].astype(F32)
            both2[block, 0, 1, here, :] = (rows_in[rows, columns].astype(F32) + added).astype(BF16)

        lax.fori_loop(0, HALF // 96, some, None)
        writing(g).start()

    run = {
        "prep": prepare, "norm": norm, "proj": project, "ret": retain, "out": give_heads,
        "mid": middle, "pass": forward, "mlp": expand, "lent": lent, "own": own_rows,
    }
    for name, _, what in ORDER:
        if name == "send":
            d, array, piece, offset, child = what
            arrive(array, piece, offset)
            source = here = chunk(array, piece, offset)
            if array in SPLIT and child == (1, 0, 0):
                source = (other_m, other_d)[array - 3].at[pl.ds(piece * PIECE_ROWS, PIECE_ROWS), :]
            pltpu.make_async_remote_copy(
                src_ref=source,
                dst_ref=here,
                send_sem=send.at[array],
                recv_sem=recv.at[slot_of(array, piece, child)],
                device_id=peers[d],
                device_id_type=MESH_ID,
            ).start()
        else:
            args, wanted = what
            for item in wanted:
                arrive(*item)
            run[name](*args)
    send_back()
    finish(len(GROUPS) - 2)
    finish(len(GROUPS) - 1)
    for array, (buffer, first, width) in enumerate(ARRAYS):
        sent = buffers[buffer].at[pl.ds(0, 31 * ROWS), pl.ds(first, width)]
        pltpu.make_async_copy(sent, sent, send.at[array]).wait()
    for g in range(len(GROUPS)):
        writing(g).wait()


def shards(
    resid, mix_gain, query_weight, key_weight, value_weight, head_gain, out_weight, mlp_gain,
    gate_weight, up_weight, down_weight,
):
    anywhere = pl.BlockSpec(memory_space=pl.ANY)
    inside = pl.BlockSpec(memory_space=pltpu.VMEM)
    return pl.pallas_call(
        layer_kernel,
        out_shape=jax.ShapeDtypeStruct((HALF, D), BF16),
        in_specs=[anywhere, inside, anywhere, anywhere, anywhere, inside, anywhere, inside, anywhere, anywhere, anywhere]
        + [inside] * 5,
        out_specs=anywhere,
        scratch_shapes=[
            pltpu.VMEM((D, 2048), BF16),
            pltpu.VMEM((D, 1024), BF16),
            pltpu.VMEM((D, ARRAYS[3][2]), BF16),
            pltpu.VMEM((D, ARRAYS[4][2]), BF16),
            pltpu.VMEM((ROWS, ARRAYS[3][2]), BF16),
            pltpu.VMEM((ROWS, ARRAYS[4][2]), BF16),
            pltpu.VMEM((2, ROWS, TILE), BF16),
            pltpu.VMEM((LEN, D), BF16),
            pltpu.VMEM((LEN, D), BF16),
            pltpu.VMEM((2, HALF, D), BF16),
            pltpu.VMEM((LEN, 2048), BF16),
            pltpu.VMEM((LEN, 1024), BF16),
            pltpu.VMEM((2, DK, DV), F32),
            pltpu.VMEM((4, HALF, SIDE + TILE), BF16),
        ]
        + [pltpu.VMEM((HALF, D), BF16)] * 3
        + [pltpu.VMEM((8, 2, 2, HALF, 256), BF16), pltpu.VMEM((8, 2, HALF, 256), BF16)]
        + [pltpu.VMEM((8, HALF, 256), BF16)] * 2
        + [
            pltpu.SemaphoreType.DMA((len(ARRAYS) * PIECES * len(OFFSETS),)),
            pltpu.SemaphoreType.DMA((len(ARRAYS),)),
            pltpu.SemaphoreType.DMA((16,)),
            pltpu.SemaphoreType.DMA((38,)),
            pltpu.SemaphoreType.DMA((38,)),
            pltpu.SemaphoreType.DMA((8,)),
        ],
        compiler_params=pltpu.CompilerParams(
            collective_id=0, has_side_effects=True, vmem_limit_bytes=67043328
        ),
    )(
        resid, mix_gain.reshape(1, -1), query_weight, key_weight, value_weight, head_gain.reshape(1, -1),
        out_weight.T, mlp_gain.reshape(1, -1), gate_weight, up_weight, down_weight.T, *tables(),
    )


def solution(mesh):
    torus = Mesh(
        mesh.devices.reshape(mesh.shape["rep"], 2, 4, 4, mesh.shape["tp"]),
        ("rep", "fs_0", "fs_1", "fs_2", "tp"),
    )
    return jax.shard_map(
        shards,
        mesh=torus,
        in_specs=(
            P(REP_FS_TP, None),
            P(),
            P(FS, "tp"),
            P(FS, "tp"),
            P(FS, "tp"),
            P("tp"),
            P("tp", FS),
            P(),
            P(FS, "tp"),
            P(FS, "tp"),
            P("tp", FS),
        ),
        out_specs=P(REP_FS_TP, None),
        check_vma=False,
    )
```

```python
import heapq

import jax
import jax.numpy as jnp
import numpy as np
from jax import lax
from jax.experimental import pallas as pl
from jax.experimental.pallas import tpu as pltpu
from jax.sharding import Mesh
from jax.sharding import PartitionSpec as P

D = 2048
DK = 256
DV = 512
BLOCK = 128
LEN = 768
HALF = LEN // 2
UNITS = 1408
FS = ("fs_0", "fs_1", "fs_2")
REP_FS_TP = ("rep", "fs_0", "fs_1", "fs_2", "tp")
MESH_ID = pl.DeviceIdType.MESH
ROWS = 64
SIDE = 640
TILE = 128
FIRST = 384
ARRAYS = ((0, 0, 1024), (0, 1024, 1024), (1, 0, 1024), (2, 0, 2 * FIRST), (2, 2 * FIRST, 640), (3, 0, SIDE + TILE))
PIECES = (4, 4, 4, 2, 2, 2)
WIDTHS = tuple(width for _, _, width in ARRAYS)
LAST = len(ARRAYS) - 1
SPLIT = (3, 4, 5)
DUE = (20, 25, 30, 66, 78, 86)
HOP = 4.0
LEAD = 4.0
OFFSETS = [(z, y, x) for z in range(2) for y in range(4) for x in range(4)]
GROUPS = [(z, y) for y in (0, 1, 3, 2) for z in range(2)]
ROOT = (0, 0, 0)
F32 = jnp.float32
BF16 = jnp.bfloat16

norm_eps = 1e-06
rope_base = 10000.0


def parent(array, piece, offset):
    z, y, x = offset
    if array in SPLIT:
        if y == x == 0:
            return (4 + piece, ROOT) if z else None
        if y and (piece == 0 or not x):
            up = y == 1 or (y == 2 and (x % 2 == 0 if piece == 0 else z == 0))
            return (2, (z, y - 1, x)) if up else (3, (z, (y + 1) % 4, x))
        up = x == 1 or (x == 2 and (y % 2 == 0 if piece == 1 else z == 0))
        return (0, (z, y, x - 1)) if up else (1, (z, y, (x + 1) % 4))
    for axis in ("zxy", "zyx", "xzy", "yzx")[piece]:
        if axis == "z" and z:
            return 4 + (x + y + piece) % 2, (0, y, x)
        if axis == "x" and x:
            up = x == 1 or (x == 2 and (piece == 1 or (piece in (0, 2) and (y + z + piece // 2) % 2 == 0)))
            return (0, (z, y, x - 1)) if up else (1, (z, y, (x + 1) % 4))
        if axis == "y" and y:
            up = y == 1 or (y == 2 and (piece == 0 or (piece in (1, 3) and (x + z) % 2 == 0)))
            return (2, (z, y - 1, x)) if up else (3, (z, (y + 1) % 4, x))
    return None


def compute_steps():
    steps = [("prep", (), (), 2.0, None), ("norm", (0,), (), 4.0, None), ("norm", (1,), (), 4.0, None)]
    steps += [("proj", (j,), (0 if j < 4 else 1,), 1.2, None) for j in range(8)]
    steps += [("ret", (t, h), (), 0.6, None) for t in range(LEN // BLOCK) for h in range(2)]
    for r in range(3):
        steps += [("out", (1, r), (2,), 2.0, None), ("out", (0, r), (), 2.0, None), ("mid", (r,), (), 0.8, None)]
    steps += [("first", (p, i), (3,), 0.9, None) for p in (0, 1) for i in range(2)]
    steps += [("pass", (i,), (), 0.1, (("mid", (i,)), 7.0 + i)) for i in range(2)]
    steps += [("first", (p, 0), (), 0.9, None) for p in (2, 3)]
    steps += [("pass", (2,), (), 0.1, (("mid", (2,)), 9.0))]
    steps += [("first", (p, 1), (), 0.9, None) for p in (2, 3)]
    steps += [("rest", (p, i), (4,), 0.8, None) for p in (2, 3, 0, 1) for i in range(2)]
    steps += [("lent", (g,), (("g", g),), 0.9, None) for g in range(8)]
    return steps + [("own", (g,), (), 0.9, None) for g in range(8)]


def program_order(steps, rate=47.0e3, latency=2.2, lead=LEAD):
    kids = {}
    for array in range(len(WIDTHS)):
        for piece in range(PIECES[array]):
            for offset in OFFSETS[1:]:
                d, above = parent(array, piece, offset)
                kids.setdefault((array, piece, above), []).append((offset, d))

    def depth(*at):
        return max([0] + [1 + depth(*at[:2], c) for c, _ in kids.get(at, [])])

    def due(array, piece, child):
        late = GROUPS.index(child[:2]) if array == LAST else 0
        return DUE[array] + late - HOP * depth(array, piece, child)

    def needs(dep):
        if isinstance(dep, tuple):
            return [(LAST, p, o) for p in range(PIECES[LAST]) for o in OFFSETS if o[:2] == GROUPS[dep[1]]]
        return [(dep, p, o) for p in range(PIECES[dep]) for o in OFFSETS]

    ready = [[] for _ in range(6)]
    free = [0.0] * 6
    coming, arrival = [], {}
    for array in range(len(WIDTHS)):
        for piece in range(PIECES[array]):
            heapq.heappush(coming, (8.0 if array in SPLIT else 2.0, (array, piece, ROOT)))
    order, now, todo, done = [], 0.0, list(steps), {}

    while todo or coming or any(ready):
        while coming and coming[0][0] <= now + 1e-9:
            at, item = heapq.heappop(coming)
            arrival[item] = at
            array, piece, offset = item
            for child, d in kids.get(item, []):
                heapq.heappush(ready[d], (due(array, piece, child), array, piece, child, offset))
        issued = False
        for d in range(6):
            while ready[d] and free[d] - now < lead:
                _, array, piece, child, offset = heapq.heappop(ready[d])
                free[d] = max(free[d], now) + WIDTHS[array] * 2 * ROWS / PIECES[array] / rate
                heapq.heappush(coming, (free[d] + latency, (array, piece, child)))
                order.append(("send", now, (d, array, piece, offset, child)))
                now += 0.03
                issued = True
        if issued:
            continue
        if todo:
            name, args, deps, cost, after = todo[0]
            start = done[after[0]] + after[1] if after else 0.0
            wanted = [c for dep in deps for c in needs(dep)]
            if now >= start and all(c in arrival for c in wanted):
                wanted.sort(key=lambda c: (arrival[c], c))
                order.append((name, now, (args, wanted)))
                now += cost
                done[name, args] = now
                todo.pop(0)
                continue
        nexts = [free[d] - lead + 1e-3 for d in range(6) if ready[d]]
        if coming:
            nexts.append(coming[0][0])
        if todo and start > now:
            nexts.append(start)
        now = max(now, min(nexts))
    return order, arrival, now, max(free)


STEPS = compute_steps()
ORDER, ARRIVAL, _, _ = program_order(STEPS)


def semaphores():
    slots, counts, onward = {}, {}, set()
    for array in range(len(ARRAYS)):
        for piece in range(PIECES[array]):
            onward |= {(array, piece, parent(array, piece, offset)[1]) for offset in OFFSETS[1:]}
    for array in range(len(ARRAYS)):
        for piece in range(PIECES[array]):
            for offset in OFFSETS[1:]:
                key = (array, piece, offset)
                if key not in onward:
                    key = (array, offset[:2] if array == LAST else None)
                counts[key] = counts.get(key, 0) + 1
                slots.setdefault(key, len(slots))
    return slots, counts


SLOTS, COUNTS = semaphores()


def tables():
    position = np.arange(LEN, dtype=np.float32)
    inverse = np.float32(1.0) / np.float32(rope_base) ** np.linspace(0.0, 1.0, DK // 2, dtype=np.float32)
    angle = position[:, None] * inverse[None, :]
    log_gamma = np.log1p(-(2.0 ** (-5.0 - 2.0 * np.arange(4))))
    offset = np.arange(BLOCK)
    distance = offset[:, None] - offset[None, :]
    inside = np.where(distance >= 0, np.exp(log_gamma[:, None, None] * np.maximum(distance, 0)), 0.0)
    query_decay = np.exp(log_gamma[:, None] * (offset + 1.0))
    key_decay = np.exp(log_gamma[:, None] * (BLOCK - 1.0 - offset))
    wide = np.ones((1, 1, BLOCK))
    found = (np.cos(angle), np.sin(angle), inside, query_decay[:, :, None] * wide, key_decay[:, :, None] * wide)
    return tuple(jnp.asarray(t.astype(np.float32)) for t in found)


def layer_kernel(
    resid, mix_gain, q_ref, k_ref, v_ref, head_gain, o_ref, mlp_gain, g_ref, u_ref, d_ref,
    cosine, sine, inside, query_decay, key_decay,
    result,
    wq, wo, wm, wd, other_m, other_d, mixed, rows_in, normed, foreign, proj, heads, state, hidden,
    keep, give, take, both2, take2, sums, back,
    recv, send, local, swap_send, swap_recv, put,
):
    buffers = (wq, wo, wm, wd)
    rep, lo, my, mx, core = (lax.axis_index(a) for a in REP_FS_TP)
    z = rep * 2 + lo
    zu, zd = lax.rem(z + 1, 4), lax.rem(z + 3, 4)
    peers = (
        {"fs_2": lax.rem(mx + 1, 4)},
        {"fs_2": lax.rem(mx + 3, 4)},
        {"fs_1": lax.rem(my + 1, 4)},
        {"fs_1": lax.rem(my + 3, 4)},
        {"rep": zu // 2, "fs_0": lax.rem(zu, 2)},
        {"rep": zd // 2, "fs_0": lax.rem(zd, 2)},
    )
    partner = {"tp": 1 - core}
    barrier = pltpu.get_barrier_semaphore()
    for peer in peers + (partner,):
        pl.semaphore_signal(barrier, inc=1, device_id=peer, device_id_type=MESH_ID)

    def base(offset):
        oz, oy, ox = offset
        owner = (lax.rem(lo + oz, 2) * 4 + lax.rem(my + 4 - oy, 4)) * 4 + lax.rem(mx + 4 - ox, 4)
        return owner * ROWS

    own = pl.ds(pl.multiple_of(base(ROOT), ROWS), ROWS)
    mine = pl.multiple_of(core * HALF, HALF)
    other = pl.multiple_of(HALF - core * HALF, HALF)
    half = (mine, other)

    ze, zb = lax.rem(z + 1 + 2 * core, 4), lax.rem(z + 3 - 2 * core, 4)
    helper = {"rep": ze // 2, "fs_0": lax.rem(ze, 2)}
    helped = {"rep": zb // 2, "fs_0": lax.rem(zb, 2)}

    def columns_of(side, first, count):
        return pl.ds(pl.multiple_of(side * (SIDE + TILE) + first, TILE), count)

    tile, shared = pl.ds(SIDE, TILE), pl.ds(2 * SIDE - 256, TILE)
    places = (((0, FIRST), 0, FIRST), ((FIRST, SIDE - FIRST), 2 * FIRST, 2 * FIRST + SIDE - FIRST + TILE))
    parts = {
        0: [(q_ref, wq.at[own, pl.ds(0, 512)]), (k_ref, wq.at[own, pl.ds(512, 512)])],
        1: [(v_ref, wq.at[own, pl.ds(1024, 1024)])],
        2: [(o_ref, wo.at[own, :])],
        3: [],
        4: [(g_ref.at[:, tile], mixed.at[0]), (u_ref.at[:, tile], mixed.at[1])],
        5: [
            (d_ref.at[:, columns_of(lo, 0, SIDE)], wd.at[own, pl.ds(0, SIDE)]),
            (d_ref.at[:, tile], wd.at[own, tile]),
            (d_ref.at[:, columns_of(1 - lo, 0, SIDE)], other_d.at[:, pl.ds(0, SIDE)]),
            (d_ref.at[:, tile], other_d.at[:, tile]),
        ],
    }
    for array, (span, gate_at, up_at) in zip((3, 4), places):
        for ref, at in ((g_ref, gate_at), (u_ref, up_at)):
            there = pl.ds(at, span[1])
            parts[array].append((ref.at[:, columns_of(lo, *span)], wm.at[own, there]))
            parts[array].append((ref.at[:, columns_of(1 - lo, *span)], other_m.at[:, there]))
    fills = {}
    for array, pairs in parts.items():
        fills[array] = []
        for source, there in pairs:
            at = sum(len(f) for f in fills.values())
            fills[array].append(pltpu.make_async_copy(source, there, local.at[at]))
            fills[array][-1].start()
    fill = pltpu.make_async_copy(resid, rows_in.at[pl.ds(mine, HALF), :], local.at[18])
    fill.start()
    pl.semaphore_wait(barrier, 7)

    def swap(source, there, slot, device=partner):
        return pltpu.make_async_remote_copy(
            src_ref=source,
            dst_ref=there,
            send_sem=swap_send.at[slot],
            recv_sem=swap_recv.at[slot],
            device_id=device,
            device_id_type=MESH_ID,
        )

    swaps = {0: swap(resid, rows_in.at[pl.ds(mine, HALF), :], 0)}
    swaps[0].start()

    def chunk(array, piece, offset):
        buffer, first, width = ARRAYS[array]
        count = ROWS // PIECES[array]
        start = pl.multiple_of(base(offset) + piece * count, count)
        return buffers[buffer].at[pl.ds(start, count), pl.ds(first, width)]

    def key_of(array, piece, offset):
        whole = (array, piece, offset)
        return whole if whole in SLOTS else (array, offset[:2] if array == LAST else None)

    waited = set()

    def arrive(array, piece, offset):
        key = (array,) if offset == ROOT else key_of(array, piece, offset)
        if key in waited:
            return
        waited.add(key)
        if offset == ROOT:
            for item in fills[array]:
                item.wait()
        else:
            buffer, first, width = ARRAYS[array]
            all_rows = COUNTS[key] * ROWS // PIECES[array]
            here = buffers[buffer].at[pl.ds(0, all_rows), pl.ds(first, width)]
            pltpu.make_async_copy(here, here, recv.at[SLOTS[key]]).wait()

    def prepare():
        arrive(4, 0, ROOT)
        lane = lax.broadcasted_iota(jnp.int32, (ROWS, TILE), 1) // (TILE // 2)
        gate = mixed[0].astype(F32)
        up = pltpu.roll(mixed[1].astype(F32), TILE // 2, 1)
        wm[own, shared] = jnp.where(lane == lo, gate, up).astype(BF16)
        other_m[:, shared] = jnp.where(lane == 1 - lo, gate, up).astype(BF16)

    def norm_rows(source, gain, start, count):
        def some(i, _):
            rows = pl.ds(pl.multiple_of(start + i * 32, 32), 32)
            wide = source[rows, :].astype(F32)
            scaled = wide * lax.rsqrt(jnp.mean(wide * wide, axis=-1, keepdims=True) + norm_eps)
            normed[rows, :] = (scaled * gain[...]).astype(BF16)

        lax.fori_loop(0, count // 32, some, None)

    def norm(which):
        if which == 0:
            fill.wait()
        else:
            swaps[0].wait()
        norm_rows(rows_in, mix_gain, half[which], HALF)

    def project(j):
        def some(i, _):
            rows = pl.ds(pl.multiple_of(i * HALF, HALF), HALF)
            columns = pl.ds(256 * j, 256)
            found = jnp.dot(normed[rows, :], wq[:, columns], preferred_element_type=F32).astype(BF16)
            if j < 4:
                wide = found.astype(F32)
                first, second = wide[:, :128], wide[:, 128:]
                c, s = cosine[rows, :], sine[rows, :]
                turned = jnp.concatenate([first * c - second * s, second * c + first * s], axis=1)
                if j >= 2:
                    turned = turned * DK**-0.5
                found = turned.astype(BF16)
            proj[rows, columns] = found

        lax.fori_loop(0, 2, some, None)

    def retain(t, h):
        rows = pl.ds(t * BLOCK, BLOCK)
        head = core * 2 + h
        queries = proj[rows, pl.ds(DK * h, DK)]
        keys = proj[rows, pl.ds(2 * DK + DK * h, DK)]
        values = proj[rows, pl.ds(4 * DK + DV * h, DV)]
        decay = query_decay[head]
        scores = lax.dot_general(queries, keys, (((1,), (1,)), ((), ())), preferred_element_type=F32)
        weights = (scores * inside[head]).astype(BF16)
        found = jnp.dot(weights, values, preferred_element_type=F32)
        if t > 0:
            carried = jnp.dot(queries, state[h].astype(BF16), preferred_element_type=F32)
            found = found + carried * jnp.concatenate([decay] * 4, axis=1)
        if t < LEN // BLOCK - 1:
            fade = key_decay[head]
            faded = (keys.astype(F32) * jnp.concatenate([fade] * 2, axis=1)).astype(BF16)
            fresh = lax.dot_general(faded, values, (((0,), (0,)), ((), ())), preferred_element_type=F32)
            if t > 0:
                last = query_decay[head, BLOCK - 1 : BLOCK, :]
                fresh = state[h] * jnp.concatenate([last] * 4, axis=1) + fresh
            state[h] = fresh
        columns = pl.ds(DV * h, DV)
        scaled = found * lax.rsqrt(jnp.mean(found * found, axis=-1, keepdims=True) + norm_eps)
        heads[rows, columns] = (scaled * head_gain[:, columns]).astype(BF16)

    third = HALF // 3

    def give_heads(which, r):
        rows = pl.ds(pl.multiple_of(half[which] + r * third, third), third)
        there = pl.ds(r * third, third)
        share = give if which else keep

        def some(j, _):
            columns = pl.ds(pl.multiple_of(j * 512, 512), 512)
            share[there, columns] = lax.dot_general(
                heads[rows, :], wo[columns, :], (((1,), (1,)), ((), ())), preferred_element_type=F32
            ).astype(BF16)

        lax.fori_loop(0, 4, some, None)
        if which:
            swaps[35 + r] = swap(give.at[there, :], take.at[there, :], 35 + r)
            swaps[35 + r].start()

    def lend(r):
        here = normed.at[pl.ds(pl.multiple_of(mine + r * third, third), third), :]
        swaps[2 + r] = swap(here, foreign.at[core, pl.ds(r * third, third), :], 2 + r, helper)
        swaps[5 + r] = swap(here, here, 5 + r)
        swaps[2 + r].start()
        swaps[5 + r].start()

    def middle(r):
        swaps[35 + r].wait()

        def some(i, _):
            here = pl.ds(pl.multiple_of(r * third + i * 32, 32), 32)
            rows = pl.ds(pl.multiple_of(mine + r * third + i * 32, 32), 32)
            added = keep[here, :].astype(F32) + take[here, :].astype(F32)
            found = (rows_in[rows, :].astype(F32) + added).astype(BF16)
            rows_in[rows, :] = found
            wide = found.astype(F32)
            scaled = wide * lax.rsqrt(jnp.mean(wide * wide, axis=-1, keepdims=True) + norm_eps)
            normed[rows, :] = (scaled * mlp_gain[...]).astype(BF16)

        lax.fori_loop(0, third // 32, some, None)
        lend(r)

    def forward(i):
        swaps[2 + i].wait()
        here = foreign.at[core, pl.ds(i * third, third), :]
        swaps[8 + i] = swap(here, here, 8 + i)
        swaps[8 + i].start()

    quarter = HALF // 2

    def rows_of(part, i):
        side = core if part % 2 == 0 else 1 - core
        if part < 2:
            source = normed[pl.ds(pl.multiple_of(side * HALF + i * quarter, quarter), quarter), :]
        else:
            source = foreign[side, pl.ds(i * quarter, quarter), :]
        return source, 2 * (part // 2) + side, pl.ds(i * quarter, quarter)

    def expand_first(part, i):
        for r in {(1, 0): (5, 6, 7), (3, 0): (8, 9), (3, 1): (10,)}.get((part, i), ()):
            swaps[r].wait()
        source, place, rows = rows_of(part, i)
        both = jnp.dot(source, wm[:, pl.ds(0, 2 * FIRST)], preferred_element_type=F32)
        hidden[place, rows, pl.ds(0, FIRST)] = (jax.nn.silu(both[:, :FIRST]) * both[:, FIRST:]).astype(BF16)

    def expand_rest(part, i):
        source, place, rows = rows_of(part, i)
        count = SIDE - FIRST
        both = jnp.dot(source, wm[:, pl.ds(2 * FIRST, 2 * count + TILE)], preferred_element_type=F32)
        hidden[place, rows, pl.ds(FIRST, count)] = (
            jax.nn.silu(both[:, :count]) * both[:, count + TILE :]
        ).astype(BF16)
        pair = both[:, count : count + TILE]
        found = jax.nn.silu(pair) * pltpu.roll(pair, TILE // 2, 1)
        lane = lax.broadcasted_iota(jnp.int32, (quarter, TILE), 1) // (TILE // 2)
        hidden[place, rows, tile] = jnp.where(lane == lo, found, 0.0).astype(BF16)

    blocks = {}

    def down_into(g, part, slot):
        block = blocks[g]
        weights = wd.at[pl.ds(pl.multiple_of(block * 256, 256), 256), :]

        def some(i, _):
            side = i * core + (1 - i) * (1 - core)
            both2[block, part, i] = lax.dot_general(
                hidden[2 * part + side], weights[...], (((1,), (1,)), ((), ())), preferred_element_type=F32
            ).astype(BF16)

        lax.fori_loop(0, 2, some, None)
        swaps[slot] = swap(both2.at[block, part, 0], take2.at[block, part], slot)
        swaps[slot].start()

    pending = []

    def send_back():
        for g in pending:
            swaps[11 + g].wait()
            block = blocks[g]

            def some(i, _, block=block):
                rows = pl.ds(pl.multiple_of(i * 96, 32), 96)
                added = both2[block, 1, 1, rows, :].astype(F32) + take2[block, 1, rows, :].astype(F32)
                sums[block, rows, :] = added.astype(BF16)

            lax.fori_loop(0, HALF // 96, some, None)
            swaps[19 + g] = swap(sums.at[block], back.at[block], 19 + g, helped)
            swaps[19 + g].start()
        pending.clear()

    def lent(g):
        oz, oy = GROUPS[g]
        blocks[g] = lax.rem(lo + oz, 2) * 4 + lax.rem(my + 4 - oy, 4)
        down_into(g, 1, 11 + g)
        send_back()
        pending.append(g)

    def own_rows(g):
        down_into(g, 0, 27 + g)
        send_back()
        if g >= 2:
            finish(g - 2)

    def writing(g):
        place = result.at[:, pl.ds(pl.multiple_of(blocks[g] * 256, 256), 256)]
        return pltpu.make_async_copy(both2.at[blocks[g], 0, 1], place, put.at[g])

    def finish(g):
        block = blocks[g]
        swaps[27 + g].wait()
        swaps[19 + g].wait_send()
        swap(sums.at[block], back.at[block], 19 + (g ^ 1), helped).wait_recv()

        def some(i, _):
            here = pl.ds(pl.multiple_of(i * 96, 32), 96)
            rows = pl.ds(pl.multiple_of(mine + i * 96, 32), 96)
            columns = pl.ds(pl.multiple_of(block * 256, 256), 256)
            added = both2[block, 0, 1, here, :].astype(F32) + take2[block, 0, here, :].astype(F32)
            added = added + back[block, here, :].astype(F32)
            both2[block, 0, 1, here, :] = (rows_in[rows, columns].astype(F32) + added).astype(BF16)

        lax.fori_loop(0, HALF // 96, some, None)
        writing(g).start()

    run = {
        "prep": prepare, "norm": norm, "proj": project, "ret": retain, "out": give_heads,
        "mid": middle, "pass": forward, "first": expand_first, "rest": expand_rest, "lent": lent, "own": own_rows,
    }
    for name, _, what in ORDER:
        if name == "send":
            d, array, piece, offset, child = what
            arrive(array, piece, offset)
            source = here = chunk(array, piece, offset)
            if array in SPLIT and child == (1, 0, 0):
                buffer, first, width = ARRAYS[array]
                count = ROWS // PIECES[array]
                source = (other_m, other_d)[buffer - 2].at[pl.ds(piece * count, count), pl.ds(first, width)]
            pltpu.make_async_remote_copy(
                src_ref=source,
                dst_ref=here,
                send_sem=send.at[array],
                recv_sem=recv.at[SLOTS[key_of(array, piece, child)]],
                device_id=peers[d],
                device_id_type=MESH_ID,
            ).start()
        else:
            args, wanted = what
            for item in sorted(wanted, key=lambda c: key_of(*c) in COUNTS and COUNTS[key_of(*c)] > 1):
                arrive(*item)
            run[name](*args)
    send_back()
    finish(len(GROUPS) - 2)
    finish(len(GROUPS) - 1)
    for array, (buffer, first, width) in enumerate(ARRAYS):
        sent = buffers[buffer].at[pl.ds(0, 31 * ROWS), pl.ds(first, width)]
        pltpu.make_async_copy(sent, sent, send.at[array]).wait()
    for g in range(len(GROUPS)):
        writing(g).wait()


def shards(
    resid, mix_gain, query_weight, key_weight, value_weight, head_gain, out_weight, mlp_gain,
    gate_weight, up_weight, down_weight,
):
    anywhere = pl.BlockSpec(memory_space=pl.ANY)
    inside = pl.BlockSpec(memory_space=pltpu.VMEM)
    return pl.pallas_call(
        layer_kernel,
        out_shape=jax.ShapeDtypeStruct((HALF, D), BF16),
        in_specs=[anywhere, inside, anywhere, anywhere, anywhere, inside, anywhere, inside, anywhere, anywhere, anywhere]
        + [inside] * 5,
        out_specs=anywhere,
        scratch_shapes=[
            pltpu.VMEM((D, 2048), BF16),
            pltpu.VMEM((D, 1024), BF16),
            pltpu.VMEM((D, 2 * SIDE + TILE), BF16),
            pltpu.VMEM((D, SIDE + TILE), BF16),
            pltpu.VMEM((ROWS, 2 * SIDE + TILE), BF16),
            pltpu.VMEM((ROWS, SIDE + TILE), BF16),
            pltpu.VMEM((2, ROWS, TILE), BF16),
            pltpu.VMEM((LEN, D), BF16),
            pltpu.VMEM((LEN, D), BF16),
            pltpu.VMEM((2, HALF, D), BF16),
            pltpu.VMEM((LEN, 2048), BF16),
            pltpu.VMEM((LEN, 1024), BF16),
            pltpu.VMEM((2, DK, DV), F32),
            pltpu.VMEM((4, HALF, SIDE + TILE), BF16),
        ]
        + [pltpu.VMEM((HALF, D), BF16)] * 3
        + [pltpu.VMEM((8, 2, 2, HALF, 256), BF16), pltpu.VMEM((8, 2, HALF, 256), BF16)]
        + [pltpu.VMEM((8, HALF, 256), BF16)] * 2
        + [
            pltpu.SemaphoreType.DMA((len(SLOTS),)),
            pltpu.SemaphoreType.DMA((len(ARRAYS),)),
            pltpu.SemaphoreType.DMA((19,)),
            pltpu.SemaphoreType.DMA((38,)),
            pltpu.SemaphoreType.DMA((38,)),
            pltpu.SemaphoreType.DMA((8,)),
        ],
        compiler_params=pltpu.CompilerParams(
            collective_id=0, has_side_effects=True, vmem_limit_bytes=67043328
        ),
    )(
        resid, mix_gain.reshape(1, -1), query_weight, key_weight, value_weight, head_gain.reshape(1, -1),
        out_weight.T, mlp_gain.reshape(1, -1), gate_weight, up_weight, down_weight.T, *tables(),
    )


def solution(mesh):
    torus = Mesh(
        mesh.devices.reshape(mesh.shape["rep"], 2, 4, 4, mesh.shape["tp"]),
        ("rep", "fs_0", "fs_1", "fs_2", "tp"),
    )
    return jax.shard_map(
        shards,
        mesh=torus,
        in_specs=(
            P(REP_FS_TP, None),
            P(),
            P(FS, "tp"),
            P(FS, "tp"),
            P(FS, "tp"),
            P("tp"),
            P("tp", FS),
            P(),
            P(FS, "tp"),
            P(FS, "tp"),
            P("tp", FS),
        ),
        out_specs=P(REP_FS_TP, None),
        check_vma=False,
    )
```

```python
import heapq

import jax
import jax.numpy as jnp
import numpy as np
from jax import lax
from jax.experimental import pallas as pl
from jax.experimental.pallas import tpu as pltpu
from jax.sharding import Mesh
from jax.sharding import PartitionSpec as P

D = 2048
DK = 256
DV = 512
BLOCK = 128
LEN = 768
HALF = LEN // 2
UNITS = 1408
FS = ("fs_0", "fs_1", "fs_2")
REP_FS_TP = ("rep", "fs_0", "fs_1", "fs_2", "tp")
MESH_ID = pl.DeviceIdType.MESH
ROWS = 64
SIDE = 640
TILE = 128
FIRST = 384
ARRAYS = ((0, 0, 1024), (0, 1024, 1024), (1, 0, 1024), (2, 0, 2 * FIRST), (2, 2 * FIRST, 640), (3, 0, SIDE + TILE))
PIECES = (4, 4, 4, 2, 2, 2)
WIDTHS = tuple(width for _, _, width in ARRAYS)
LAST = len(ARRAYS) - 1
SPLIT = (3, 4, 5)
EVEN = ("zxy", "zyx", "xzy", "yzx")
TREES = (EVEN, EVEN, EVEN)
DUE = (20, 25, 30, 70, 72, 110)
HOP = 4.0
CROSS = 30.0
LEAD = 4.0
OFFSETS = [(z, y, x) for z in range(2) for y in range(4) for x in range(4)]
GROUPS = [(z, y) for y in (0, 1, 3, 2) for z in range(2)]
ROOT = (0, 0, 0)
F32 = jnp.float32
BF16 = jnp.bfloat16

norm_eps = 1e-06
rope_base = 10000.0


def parent(array, piece, offset):
    z, y, x = offset
    if array in SPLIT:
        if y == x == 0:
            return (4 + piece, ROOT) if z else None
        if y and (piece == 0 or not x):
            up = y == 1 or (y == 2 and (x % 2 == 0 if piece == 0 else z == 0))
            return (2, (z, y - 1, x)) if up else (3, (z, (y + 1) % 4, x))
        up = x == 1 or (x == 2 and (y % 2 == 0 if piece == 1 else z == 0))
        return (0, (z, y, x - 1)) if up else (1, (z, y, (x + 1) % 4))
    for axis in TREES[array][piece]:
        if axis == "z" and z:
            return 4 + (x + y + piece) % 2, (0, y, x)
        if axis == "x" and x:
            up = x == 1 or (x == 2 and (piece == 1 or (piece in (0, 2) and (y + z + piece // 2) % 2 == 0)))
            return (0, (z, y, x - 1)) if up else (1, (z, y, (x + 1) % 4))
        if axis == "y" and y:
            up = y == 1 or (y == 2 and (piece == 0 or (piece in (1, 3) and (x + z) % 2 == 0)))
            return (2, (z, y - 1, x)) if up else (3, (z, (y + 1) % 4, x))
    return None


def compute_steps():
    steps = [("prep", (), (), 2.0, None), ("norm", (0,), (), 4.0, None), ("norm", (1,), (), 4.0, None)]
    steps += [("proj", (j,), (0 if j < 4 else 1,), 1.2, None) for j in range(8)]
    steps += [("ret", (t, h), (), 0.6, None) for t in range(LEN // BLOCK) for h in range(2)]
    for r in range(3):
        steps += [("out", (1, r), (2,), 2.0, None), ("out", (0, r), (), 2.0, None), ("mid", (r,), (), 0.8, None)]
    own = [("first", (p, i), (3,), 1.0, None) for p in (0, 1) for i in range(2)]
    passes = [("pass", (i,), (), 0.1, (("mid", (i,)), 7.0 + i)) for i in range(3)]
    steps += passes[:2] + [("first", (p, 0), (3,), 1.0, None) for p in (2, 3)] + own + passes[2:]
    steps += [("first", (p, 1), (), 1.0, None) for p in (2, 3)]
    steps += [("rest", (p, i), (4,), 0.9, None) for p in (2, 3) for i in range(2)]
    own = [("rest", (p, i), (), 0.9, None) for p in (0, 1) for i in range(2)]
    for g in range(8):
        steps += [("lent", (g,), (("g", g),), 1.1, None)] + own[g : g + 1]
    return steps + [("own", (g,), (), 0.9, None) for g in range(8)]


def program_order(steps, rate=47.0e3, latency=2.2, lead=LEAD):
    kids = {}
    for array in range(len(WIDTHS)):
        for piece in range(PIECES[array]):
            for offset in OFFSETS[1:]:
                d, above = parent(array, piece, offset)
                kids.setdefault((array, piece, above), []).append((offset, d))

    def depth(*at):
        return max([0] + [1 + depth(*at[:2], c) for c, _ in kids.get(at, [])])

    def due(array, piece, child):
        if array in SPLIT and child == (1, 0, 0):
            return CROSS
        late = GROUPS.index(child[:2]) if array == LAST else 0
        return DUE[array] + late - HOP * depth(array, piece, child)

    def needs(dep):
        if isinstance(dep, tuple):
            return [(LAST, p, o) for p in range(PIECES[LAST]) for o in OFFSETS if o[:2] == GROUPS[dep[1]]]
        return [(dep, p, o) for p in range(PIECES[dep]) for o in OFFSETS]

    ready = [[] for _ in range(6)]
    free = [0.0] * 6
    coming, arrival = [], {}
    for array in range(len(WIDTHS)):
        for piece in range(PIECES[array]):
            heapq.heappush(coming, (8.0 if array in SPLIT else 2.0, (array, piece, ROOT)))
    order, now, todo, done = [], 0.0, list(steps), {}

    while todo or coming or any(ready):
        while coming and coming[0][0] <= now + 1e-9:
            at, item = heapq.heappop(coming)
            arrival[item] = at
            array, piece, offset = item
            for child, d in kids.get(item, []):
                heapq.heappush(ready[d], (due(array, piece, child), array, piece, child, offset))
        issued = False
        for d in range(6):
            while ready[d] and free[d] - now < lead:
                _, array, piece, child, offset = heapq.heappop(ready[d])
                free[d] = max(free[d], now) + WIDTHS[array] * 2 * ROWS / PIECES[array] / rate
                heapq.heappush(coming, (free[d] + latency, (array, piece, child)))
                order.append(("send", now, (d, array, piece, offset, child)))
                now += 0.03
                issued = True
        if issued:
            continue
        if todo:
            name, args, deps, cost, after = todo[0]
            start = done[after[0]] + after[1] if after else 0.0
            wanted = [c for dep in deps for c in needs(dep)]
            if now >= start and all(c in arrival for c in wanted):
                wanted.sort(key=lambda c: (arrival[c], c))
                order.append((name, now, (args, wanted)))
                now += cost
                done[name, args] = now
                todo.pop(0)
                continue
        nexts = [free[d] - lead + 1e-3 for d in range(6) if ready[d]]
        if coming:
            nexts.append(coming[0][0])
        if todo and start > now:
            nexts.append(start)
        now = max(now, min(nexts))
    return order, arrival, now, max(free)


STEPS = compute_steps()
ORDER, ARRIVAL, _, _ = program_order(STEPS)


def semaphores():
    slots, counts, onward = {}, {}, set()
    for array in range(len(ARRAYS)):
        for piece in range(PIECES[array]):
            onward |= {(array, piece, parent(array, piece, offset)[1]) for offset in OFFSETS[1:]}
    for array in range(len(ARRAYS)):
        for piece in range(PIECES[array]):
            for offset in OFFSETS[1:]:
                key = (array, piece, offset)
                if key not in onward:
                    key = (array, offset[:2] if array == LAST else None)
                counts[key] = counts.get(key, 0) + 1
                slots.setdefault(key, len(slots))
    return slots, counts


SLOTS, COUNTS = semaphores()


def tables():
    position = np.arange(LEN, dtype=np.float32)
    inverse = np.float32(1.0) / np.float32(rope_base) ** np.linspace(0.0, 1.0, DK // 2, dtype=np.float32)
    angle = position[:, None] * inverse[None, :]
    log_gamma = np.log1p(-(2.0 ** (-5.0 - 2.0 * np.arange(4))))
    offset = np.arange(BLOCK)
    distance = offset[:, None] - offset[None, :]
    inside = np.where(distance >= 0, np.exp(log_gamma[:, None, None] * np.maximum(distance, 0)), 0.0)
    query_decay = np.exp(log_gamma[:, None] * (offset + 1.0))
    key_decay = np.exp(log_gamma[:, None] * (BLOCK - 1.0 - offset))
    wide = np.ones((1, 1, BLOCK))
    found = (np.cos(angle), np.sin(angle), inside, query_decay[:, :, None] * wide, key_decay[:, :, None] * wide)
    return tuple(jnp.asarray(t.astype(np.float32)) for t in found)


def layer_kernel(
    resid, mix_gain, q_ref, k_ref, v_ref, head_gain, o_ref, mlp_gain, g_ref, u_ref, d_ref,
    cosine, sine, inside, query_decay, key_decay,
    result,
    wq, wo, wm, wd, other_m, other_d, mixed, rows_in, normed, foreign, proj, heads, state, hidden,
    keep, give, take, both2, take2, sums, back,
    recv, send, local, swap_send, swap_recv, put,
):
    buffers = (wq, wo, wm, wd)
    rep, lo, my, mx, core = (lax.axis_index(a) for a in REP_FS_TP)
    z = rep * 2 + lo
    zu, zd = lax.rem(z + 1, 4), lax.rem(z + 3, 4)
    peers = (
        {"fs_2": lax.rem(mx + 1, 4)},
        {"fs_2": lax.rem(mx + 3, 4)},
        {"fs_1": lax.rem(my + 1, 4)},
        {"fs_1": lax.rem(my + 3, 4)},
        {"rep": zu // 2, "fs_0": lax.rem(zu, 2)},
        {"rep": zd // 2, "fs_0": lax.rem(zd, 2)},
    )
    partner = {"tp": 1 - core}
    barrier = pltpu.get_barrier_semaphore()
    for peer in peers + (partner,):
        pl.semaphore_signal(barrier, inc=1, device_id=peer, device_id_type=MESH_ID)

    def base(offset):
        oz, oy, ox = offset
        owner = (lax.rem(lo + oz, 2) * 4 + lax.rem(my + 4 - oy, 4)) * 4 + lax.rem(mx + 4 - ox, 4)
        return owner * ROWS

    own = pl.ds(pl.multiple_of(base(ROOT), ROWS), ROWS)
    mine = pl.multiple_of(core * HALF, HALF)
    other = pl.multiple_of(HALF - core * HALF, HALF)
    half = (mine, other)

    ze, zb = lax.rem(z + 1 + 2 * core, 4), lax.rem(z + 3 - 2 * core, 4)
    helper = {"rep": ze // 2, "fs_0": lax.rem(ze, 2)}
    helped = {"rep": zb // 2, "fs_0": lax.rem(zb, 2)}

    def columns_of(side, first, count):
        return pl.ds(pl.multiple_of(side * (SIDE + TILE) + first, TILE), count)

    tile, shared = pl.ds(SIDE, TILE), pl.ds(2 * SIDE - 256, TILE)
    places = (((0, FIRST), 0, FIRST), ((FIRST, SIDE - FIRST), 2 * FIRST, 2 * FIRST + SIDE - FIRST + TILE))
    parts = {
        0: [(q_ref, wq.at[own, pl.ds(0, 512)]), (k_ref, wq.at[own, pl.ds(512, 512)])],
        1: [(v_ref, wq.at[own, pl.ds(1024, 1024)])],
        2: [(o_ref, wo.at[own, :])],
        3: [],
        4: [(g_ref.at[:, tile], mixed.at[0]), (u_ref.at[:, tile], mixed.at[1])],
        5: [
            (d_ref.at[:, columns_of(lo, 0, SIDE)], wd.at[own, pl.ds(0, SIDE)]),
            (d_ref.at[:, tile], wd.at[own, tile]),
            (d_ref.at[:, columns_of(1 - lo, 0, SIDE)], other_d.at[:, pl.ds(0, SIDE)]),
            (d_ref.at[:, tile], other_d.at[:, tile]),
        ],
    }
    for array, (span, gate_at, up_at) in zip((3, 4), places):
        for ref, at in ((g_ref, gate_at), (u_ref, up_at)):
            there = pl.ds(at, span[1])
            parts[array].append((ref.at[:, columns_of(lo, *span)], wm.at[own, there]))
            parts[array].append((ref.at[:, columns_of(1 - lo, *span)], other_m.at[:, there]))
    fills = {}
    for array, pairs in parts.items():
        fills[array] = []
        for source, there in pairs:
            at = sum(len(f) for f in fills.values())
            fills[array].append(pltpu.make_async_copy(source, there, local.at[at]))
            fills[array][-1].start()
    fill = pltpu.make_async_copy(resid, rows_in.at[pl.ds(mine, HALF), :], local.at[18])
    fill.start()
    pl.semaphore_wait(barrier, 7)

    def swap(source, there, slot, device=partner):
        return pltpu.make_async_remote_copy(
            src_ref=source,
            dst_ref=there,
            send_sem=swap_send.at[0 if slot < 11 else 1],
            recv_sem=swap_recv.at[slot],
            device_id=device,
            device_id_type=MESH_ID,
        )

    swaps = {0: swap(resid, rows_in.at[pl.ds(mine, HALF), :], 0)}
    swaps[0].start()

    def chunk(array, piece, offset):
        buffer, first, width = ARRAYS[array]
        count = ROWS // PIECES[array]
        start = pl.multiple_of(base(offset) + piece * count, count)
        return buffers[buffer].at[pl.ds(start, count), pl.ds(first, width)]

    def key_of(array, piece, offset):
        whole = (array, piece, offset)
        return whole if whole in SLOTS else (array, offset[:2] if array == LAST else None)

    waited = set()

    def arrive(array, piece, offset):
        key = (array,) if offset == ROOT else key_of(array, piece, offset)
        if key in waited:
            return
        waited.add(key)
        if offset == ROOT:
            for item in fills[array]:
                item.wait()
        else:
            buffer, first, width = ARRAYS[array]
            all_rows = COUNTS[key] * ROWS // PIECES[array]
            here = buffers[buffer].at[pl.ds(0, all_rows), pl.ds(first, width)]
            pltpu.make_async_copy(here, here, recv.at[SLOTS[key]]).wait()

    def prepare():
        arrive(4, 0, ROOT)
        lane = lax.broadcasted_iota(jnp.int32, (ROWS, TILE), 1) // (TILE // 2)
        gate = mixed[0].astype(F32)
        up = pltpu.roll(mixed[1].astype(F32), TILE // 2, 1)
        wm[own, shared] = jnp.where(lane == lo, gate, up).astype(BF16)
        other_m[:, shared] = jnp.where(lane == 1 - lo, gate, up).astype(BF16)

    def norm_rows(source, gain, start, count):
        def some(i, _):
            rows = pl.ds(pl.multiple_of(start + i * 32, 32), 32)
            wide = source[rows, :].astype(F32)
            scaled = wide * lax.rsqrt(jnp.mean(wide * wide, axis=-1, keepdims=True) + norm_eps)
            normed[rows, :] = (scaled * gain[...]).astype(BF16)

        lax.fori_loop(0, count // 32, some, None)

    def norm(which):
        if which == 0:
            fill.wait()
        else:
            swaps[0].wait_recv()
        norm_rows(rows_in, mix_gain, half[which], HALF)

    def project(j):
        def some(i, _):
            rows = pl.ds(pl.multiple_of(i * HALF, HALF), HALF)
            columns = pl.ds(256 * j, 256)
            found = jnp.dot(normed[rows, :], wq[:, columns], preferred_element_type=F32).astype(BF16)
            if j < 4:
                wide = found.astype(F32)
                first, second = wide[:, :128], wide[:, 128:]
                c, s = cosine[rows, :], sine[rows, :]
                turned = jnp.concatenate([first * c - second * s, second * c + first * s], axis=1)
                if j >= 2:
                    turned = turned * DK**-0.5
                found = turned.astype(BF16)
            proj[rows, columns] = found

        lax.fori_loop(0, 2, some, None)

    def retain(t, h):
        rows = pl.ds(t * BLOCK, BLOCK)
        head = core * 2 + h
        queries = proj[rows, pl.ds(DK * h, DK)]
        keys = proj[rows, pl.ds(2 * DK + DK * h, DK)]
        values = proj[rows, pl.ds(4 * DK + DV * h, DV)]
        decay = query_decay[head]
        scores = lax.dot_general(queries, keys, (((1,), (1,)), ((), ())), preferred_element_type=F32)
        weights = (scores * inside[head]).astype(BF16)
        found = jnp.dot(weights, values, preferred_element_type=F32)
        if t > 0:
            carried = jnp.dot(queries, state[h].astype(BF16), preferred_element_type=F32)
            found = found + carried * jnp.concatenate([decay] * 4, axis=1)
        if t < LEN // BLOCK - 1:
            fade = key_decay[head]
            faded = (keys.astype(F32) * jnp.concatenate([fade] * 2, axis=1)).astype(BF16)
            fresh = lax.dot_general(faded, values, (((0,), (0,)), ((), ())), preferred_element_type=F32)
            if t > 0:
                last = query_decay[head, BLOCK - 1 : BLOCK, :]
                fresh = state[h] * jnp.concatenate([last] * 4, axis=1) + fresh
            state[h] = fresh
        columns = pl.ds(DV * h, DV)
        scaled = found * lax.rsqrt(jnp.mean(found * found, axis=-1, keepdims=True) + norm_eps)
        heads[rows, columns] = (scaled * head_gain[:, columns]).astype(BF16)

    third = HALF // 3

    def give_heads(which, r):
        rows = pl.ds(pl.multiple_of(half[which] + r * third, third), third)
        there = pl.ds(r * third, third)
        share = give if which else keep

        def some(j, _):
            columns = pl.ds(pl.multiple_of(j * 512, 512), 512)
            share[there, columns] = lax.dot_general(
                heads[rows, :], wo[columns, :], (((1,), (1,)), ((), ())), preferred_element_type=F32
            ).astype(BF16)

        lax.fori_loop(0, 4, some, None)
        if which:
            swaps[35 + r] = swap(give.at[there, :], take.at[there, :], 35 + r)
            swaps[35 + r].start()

    def lend(r):
        here = normed.at[pl.ds(pl.multiple_of(mine + r * third, third), third), :]
        swaps[2 + r] = swap(here, foreign.at[core, pl.ds(r * third, third), :], 2 + r, helper)
        swaps[5 + r] = swap(here, here, 5 + r)
        swaps[2 + r].start()
        swaps[5 + r].start()

    def middle(r):
        swaps[35 + r].wait_recv()

        def some(i, _):
            here = pl.ds(pl.multiple_of(r * third + i * 32, 32), 32)
            rows = pl.ds(pl.multiple_of(mine + r * third + i * 32, 32), 32)
            added = keep[here, :].astype(F32) + take[here, :].astype(F32)
            found = (rows_in[rows, :].astype(F32) + added).astype(BF16)
            rows_in[rows, :] = found
            wide = found.astype(F32)
            scaled = wide * lax.rsqrt(jnp.mean(wide * wide, axis=-1, keepdims=True) + norm_eps)
            normed[rows, :] = (scaled * mlp_gain[...]).astype(BF16)

        lax.fori_loop(0, third // 32, some, None)
        lend(r)

    def forward(i):
        swaps[2 + i].wait_recv()
        here = foreign.at[core, pl.ds(i * third, third), :]
        swaps[8 + i] = swap(here, here, 8 + i)
        swaps[8 + i].start()

    quarter = HALF // 2

    def rows_of(part, i):
        side = core if part % 2 == 0 else 1 - core
        if part < 2:
            source = normed[pl.ds(pl.multiple_of(side * HALF + i * quarter, quarter), quarter), :]
        else:
            source = foreign[side, pl.ds(i * quarter, quarter), :]
        return source, 2 * (part // 2) + side, pl.ds(i * quarter, quarter)

    def expand_first(part, i):
        for r in {(1, 0): (5, 6, 7), (3, 0): (8, 9), (3, 1): (10,)}.get((part, i), ()):
            swaps[r].wait_recv()
        source, place, rows = rows_of(part, i)
        both = jnp.dot(source, wm[:, pl.ds(0, 2 * FIRST)], preferred_element_type=F32)
        hidden[place, rows, pl.ds(0, FIRST)] = (jax.nn.silu(both[:, :FIRST]) * both[:, FIRST:]).astype(BF16)

    def expand_rest(part, i):
        source, place, rows = rows_of(part, i)
        count = SIDE - FIRST
        both = jnp.dot(source, wm[:, pl.ds(2 * FIRST, 2 * count + TILE)], preferred_element_type=F32)
        hidden[place, rows, pl.ds(FIRST, count)] = (
            jax.nn.silu(both[:, :count]) * both[:, count + TILE :]
        ).astype(BF16)
        pair = both[:, count : count + TILE]
        found = jax.nn.silu(pair) * pltpu.roll(pair, TILE // 2, 1)
        lane = lax.broadcasted_iota(jnp.int32, (quarter, TILE), 1) // (TILE // 2)
        hidden[place, rows, tile] = jnp.where(lane == lo, found, 0.0).astype(BF16)
        send_back()

    blocks = {}

    def down_into(g, part, slot):
        block = blocks[g]
        weights = wd.at[pl.ds(pl.multiple_of(block * 256, 256), 256), :]

        def some(i, _):
            side = i * core + (1 - i) * (1 - core)
            both2[block, part, i] = lax.dot_general(
                hidden[2 * part + side], weights[...], (((1,), (1,)), ((), ())), preferred_element_type=F32
            ).astype(BF16)

        lax.fori_loop(0, 2, some, None)
        swaps[slot] = swap(both2.at[block, part, 0], take2.at[block, part], slot)
        swaps[slot].start()

    pending = []

    def send_back():
        for g in pending:
            swaps[11 + g].wait_recv()
            block = blocks[g]

            def some(i, _, block=block):
                rows = pl.ds(pl.multiple_of(i * 96, 32), 96)
                added = both2[block, 1, 1, rows, :].astype(F32) + take2[block, 1, rows, :].astype(F32)
                sums[block, rows, :] = added.astype(BF16)

            lax.fori_loop(0, HALF // 96, some, None)
            swaps[19 + g] = swap(sums.at[block], back.at[block], 19 + g, helped)
            swaps[19 + g].start()
        pending.clear()

    def lent(g):
        oz, oy = GROUPS[g]
        blocks[g] = lax.rem(lo + oz, 2) * 4 + lax.rem(my + 4 - oy, 4)
        down_into(g, 1, 11 + g)
        send_back()
        pending.append(g)

    def own_rows(g):
        down_into(g, 0, 27 + g)
        send_back()
        if g >= 2:
            finish(g - 2)

    def writing(g):
        place = result.at[:, pl.ds(pl.multiple_of(blocks[g] * 256, 256), 256)]
        return pltpu.make_async_copy(both2.at[blocks[g], 0, 1], place, put.at[0])

    def finish(g):
        block = blocks[g]
        swaps[27 + g].wait_recv()
        swap(sums.at[block], back.at[block], 19 + (g ^ 1), helped).wait_recv()

        def some(i, _):
            here = pl.ds(pl.multiple_of(i * 96, 32), 96)
            rows = pl.ds(pl.multiple_of(mine + i * 96, 32), 96)
            columns = pl.ds(pl.multiple_of(block * 256, 256), 256)
            added = both2[block, 0, 1, here, :].astype(F32) + take2[block, 0, here, :].astype(F32)
            added = added + back[block, here, :].astype(F32)
            both2[block, 0, 1, here, :] = (rows_in[rows, columns].astype(F32) + added).astype(BF16)

        lax.fori_loop(0, HALF // 96, some, None)
        writing(g).start()

    run = {
        "prep": prepare, "norm": norm, "proj": project, "ret": retain, "out": give_heads,
        "mid": middle, "pass": forward, "first": expand_first, "rest": expand_rest, "lent": lent, "own": own_rows,
    }
    for name, _, what in ORDER:
        if name == "send":
            d, array, piece, offset, child = what
            arrive(array, piece, offset)
            source = here = chunk(array, piece, offset)
            if array in SPLIT and child == (1, 0, 0):
                buffer, first, width = ARRAYS[array]
                count = ROWS // PIECES[array]
                source = (other_m, other_d)[buffer - 2].at[pl.ds(piece * count, count), pl.ds(first, width)]
            pltpu.make_async_remote_copy(
                src_ref=source,
                dst_ref=here,
                send_sem=send.at[array],
                recv_sem=recv.at[SLOTS[key_of(array, piece, child)]],
                device_id=peers[d],
                device_id_type=MESH_ID,
            ).start()
        else:
            args, wanted = what
            for item in sorted(wanted, key=lambda c: key_of(*c) in COUNTS and COUNTS[key_of(*c)] > 1):
                arrive(*item)
            run[name](*args)
    send_back()
    finish(len(GROUPS) - 2)
    finish(len(GROUPS) - 1)
    for array, (buffer, first, width) in enumerate(ARRAYS):
        sent = buffers[buffer].at[pl.ds(0, 31 * ROWS), pl.ds(first, width)]
        pltpu.make_async_copy(sent, sent, send.at[array]).wait()
    for slot in range(2):
        pltpu.make_async_copy(both2, both2, swap_send.at[slot]).wait()
    pltpu.make_async_copy(result, result, put.at[0]).wait()


def shards(
    resid, mix_gain, query_weight, key_weight, value_weight, head_gain, out_weight, mlp_gain,
    gate_weight, up_weight, down_weight,
):
    anywhere = pl.BlockSpec(memory_space=pl.ANY)
    inside = pl.BlockSpec(memory_space=pltpu.VMEM)
    return pl.pallas_call(
        layer_kernel,
        out_shape=jax.ShapeDtypeStruct((HALF, D), BF16),
        in_specs=[anywhere, inside, anywhere, anywhere, anywhere, inside, anywhere, inside, anywhere, anywhere, anywhere]
        + [inside] * 5,
        out_specs=anywhere,
        scratch_shapes=[
            pltpu.VMEM((D, 2048), BF16),
            pltpu.VMEM((D, 1024), BF16),
            pltpu.VMEM((D, 2 * SIDE + TILE), BF16),
            pltpu.VMEM((D, SIDE + TILE), BF16),
            pltpu.VMEM((ROWS, 2 * SIDE + TILE), BF16),
            pltpu.VMEM((ROWS, SIDE + TILE), BF16),
            pltpu.VMEM((2, ROWS, TILE), BF16),
            pltpu.VMEM((LEN, D), BF16),
            pltpu.VMEM((LEN, D), BF16),
            pltpu.VMEM((2, HALF, D), BF16),
            pltpu.VMEM((LEN, 2048), BF16),
            pltpu.VMEM((LEN, 1024), BF16),
            pltpu.VMEM((2, DK, DV), F32),
            pltpu.VMEM((4, HALF, SIDE + TILE), BF16),
        ]
        + [pltpu.VMEM((HALF, D), BF16)] * 3
        + [pltpu.VMEM((8, 2, 2, HALF, 256), BF16), pltpu.VMEM((8, 2, HALF, 256), BF16)]
        + [pltpu.VMEM((8, HALF, 256), BF16)] * 2
        + [
            pltpu.SemaphoreType.DMA((len(SLOTS),)),
            pltpu.SemaphoreType.DMA((len(ARRAYS),)),
            pltpu.SemaphoreType.DMA((19,)),
            pltpu.SemaphoreType.DMA((2,)),
            pltpu.SemaphoreType.DMA((38,)),
            pltpu.SemaphoreType.DMA((1,)),
        ],
        compiler_params=pltpu.CompilerParams(
            collective_id=0, has_side_effects=True, vmem_limit_bytes=67043328
        ),
    )(
        resid, mix_gain.reshape(1, -1), query_weight, key_weight, value_weight, head_gain.reshape(1, -1),
        out_weight.T, mlp_gain.reshape(1, -1), gate_weight, up_weight, down_weight.T, *tables(),
    )


def solution(mesh):
    torus = Mesh(
        mesh.devices.reshape(mesh.shape["rep"], 2, 4, 4, mesh.shape["tp"]),
        ("rep", "fs_0", "fs_1", "fs_2", "tp"),
    )
    return jax.shard_map(
        shards,
        mesh=torus,
        in_specs=(
            P(REP_FS_TP, None),
            P(),
            P(FS, "tp"),
            P(FS, "tp"),
            P(FS, "tp"),
            P("tp"),
            P("tp", FS),
            P(),
            P(FS, "tp"),
            P(FS, "tp"),
            P("tp", FS),
        ),
        out_specs=P(REP_FS_TP, None),
        check_vma=False,
    )
```

```python
import heapq

import jax
import jax.numpy as jnp
import numpy as np
from jax import lax
from jax.experimental import pallas as pl
from jax.experimental.pallas import tpu as pltpu
from jax.sharding import Mesh
from jax.sharding import PartitionSpec as P

D = 2048
DK = 256
DV = 512
BLOCK = 128
LEN = 768
HALF = LEN // 2
UNITS = 1408
FS = ("fs_0", "fs_1", "fs_2")
REP_FS_TP = ("rep", "fs_0", "fs_1", "fs_2", "tp")
MESH_ID = pl.DeviceIdType.MESH
ROWS = 64
SIDE = 640
TILE = 128
FIRST = 256
ARRAYS = ((0, 0, 1024), (0, 1024, 1024), (1, 0, 1024), (2, 0, 2 * FIRST), (2, 2 * FIRST, 2 * (SIDE - FIRST) + TILE), (3, 0, SIDE + TILE))
PIECES = (4, 4, 4, 2, 2, 2)
WIDTHS = tuple(width for _, _, width in ARRAYS)
LAST = len(ARRAYS) - 1
SPLIT = (3, 4, 5)
EVEN = ("zxy", "zyx", "xzy", "yzx")
TREES = (EVEN, EVEN, EVEN)
DUE = (20, 25, 30, 60, 60, 85)
HOP = 4.0
CROSS = 30.0
LEAD = 3.0
OFFSETS = [(z, y, x) for z in range(2) for y in range(4) for x in range(4)]
GROUPS = [(z, y) for y in (0, 1, 3, 2) for z in range(2)]
ROOT = (0, 0, 0)
F32 = jnp.float32
BF16 = jnp.bfloat16

norm_eps = 1e-06
rope_base = 10000.0


def parent(array, piece, offset):
    z, y, x = offset
    if array in SPLIT:
        if y == x == 0:
            return (4 + piece, ROOT) if z else None
        if y and (piece == 0 or not x):
            up = y == 1 or (y == 2 and (x % 2 == 0 if piece == 0 else z == 0))
            return (2, (z, y - 1, x)) if up else (3, (z, (y + 1) % 4, x))
        up = x == 1 or (x == 2 and (y % 2 == 0 if piece == 1 else z == 0))
        return (0, (z, y, x - 1)) if up else (1, (z, y, (x + 1) % 4))
    for axis in TREES[array][piece]:
        if axis == "z" and z:
            return 4 + (x + y + piece) % 2, (0, y, x)
        if axis == "x" and x:
            up = x == 1 or (x == 2 and (piece == 1 or (piece in (0, 2) and (y + z + piece // 2) % 2 == 0)))
            return (0, (z, y, x - 1)) if up else (1, (z, y, (x + 1) % 4))
        if axis == "y" and y:
            up = y == 1 or (y == 2 and (piece == 0 or (piece in (1, 3) and (x + z) % 2 == 0)))
            return (2, (z, y - 1, x)) if up else (3, (z, (y + 1) % 4, x))
    return None


def compute_steps():
    steps = [("prep", (), (), 2.0, None), ("norm", (0,), (), 4.0, None), ("norm", (1,), (), 4.0, None)]
    steps += [("proj", (j,), (0 if j < 4 else 1,), 1.2, None) for j in range(8)]
    steps += [("ret", (t, h), (), 0.6, None) for t in range(LEN // BLOCK) for h in range(2)]
    for r in range(3):
        steps += [("out", (1, r), (2,), 2.0, None), ("out", (0, r), (), 2.0, None), ("mid", (r,), (), 0.8, None)]
    def part(name, parts, half, us, deps=()):
        return [(name, (p, i), deps, us, None) for p in parts for i in half]

    passes = [("pass", (i,), (), 0.1, (("mid", (i,)), (7.0, 8.3, 8.5)[i])) for i in range(3)]
    steps += passes[:1] + part("first", (0, 1), (0, 1), 0.8, (3,)) + passes[1:2]
    steps += part("first", (2, 3), (0,), 0.8) + passes[2:] + part("first", (2, 3), (1,), 0.9)
    steps += part("rest", (2, 3), (0, 1), 1.05, (4,))
    own = part("rest", (0, 1), (0, 1), 1.05)
    for g in range(8):
        steps += [("lent", (g,), (("g", g),), 1.1, None)] + own[g : g + 1]
    return steps + [("own", (g,), (), 0.9, None) for g in range(8)]


def program_order(steps, rate=46.0e3, latency=2.2, lead=LEAD):
    kids = {}
    for array in range(len(WIDTHS)):
        for piece in range(PIECES[array]):
            for offset in OFFSETS[1:]:
                d, above = parent(array, piece, offset)
                kids.setdefault((array, piece, above), []).append((offset, d))

    def depth(*at):
        return max([0] + [1 + depth(*at[:2], c) for c, _ in kids.get(at, [])])

    def due(array, piece, child):
        if array in SPLIT and child == (1, 0, 0):
            return CROSS
        late = GROUPS.index(child[:2]) if array == LAST else 0
        return DUE[array] + late - HOP * depth(array, piece, child)

    def needs(dep):
        if isinstance(dep, tuple):
            return [(LAST, p, o) for p in range(PIECES[LAST]) for o in OFFSETS if o[:2] == GROUPS[dep[1]]]
        return [(dep, p, o) for p in range(PIECES[dep]) for o in OFFSETS]

    ready = [[] for _ in range(6)]
    free = [0.0] * 6
    coming, arrival = [], {}
    for array in range(len(WIDTHS)):
        for piece in range(PIECES[array]):
            heapq.heappush(coming, (8.0 if array in SPLIT else 2.0, (array, piece, ROOT)))
    order, now, todo, done = [], 0.0, list(steps), {}

    while todo or coming or any(ready):
        while coming and coming[0][0] <= now + 1e-9:
            at, item = heapq.heappop(coming)
            arrival[item] = at
            array, piece, offset = item
            for child, d in kids.get(item, []):
                heapq.heappush(ready[d], (due(array, piece, child), array, piece, child, offset))
        issued = False
        for d in range(6):
            while ready[d] and free[d] - now < lead:
                _, array, piece, child, offset = heapq.heappop(ready[d])
                free[d] = max(free[d], now) + WIDTHS[array] * 2 * ROWS / PIECES[array] / rate
                heapq.heappush(coming, (free[d] + latency, (array, piece, child)))
                order.append(("send", now, (d, array, piece, offset, child)))
                now += 0.03
                issued = True
        if issued:
            continue
        if todo:
            name, args, deps, cost, after = todo[0]
            start = done[after[0]] + after[1] if after else 0.0
            wanted = [c for dep in deps for c in needs(dep)]
            if now >= start and all(c in arrival for c in wanted):
                wanted.sort(key=lambda c: (arrival[c], c))
                order.append((name, now, (args, wanted)))
                now += cost
                done[name, args] = now
                todo.pop(0)
                continue
        nexts = [free[d] - lead + 1e-3 for d in range(6) if ready[d]]
        if coming:
            nexts.append(coming[0][0])
        if todo and start > now:
            nexts.append(start)
        now = max(now, min(nexts))
    return order, arrival, now, max(free)


STEPS = compute_steps()
ORDER, ARRIVAL, _, _ = program_order(STEPS)


def semaphores():
    slots, counts, onward = {}, {}, set()
    for array in range(len(ARRAYS)):
        for piece in range(PIECES[array]):
            onward |= {(array, piece, parent(array, piece, offset)[1]) for offset in OFFSETS[1:]}
    for array in range(len(ARRAYS)):
        for piece in range(PIECES[array]):
            for offset in OFFSETS[1:]:
                key = (array, piece, offset)
                if key not in onward:
                    key = (array, offset[:2] if array == LAST else None)
                counts[key] = counts.get(key, 0) + 1
                slots.setdefault(key, len(slots))
    return slots, counts


SLOTS, COUNTS = semaphores()


def tables():
    position = np.arange(LEN, dtype=np.float32)
    inverse = np.float32(1.0) / np.float32(rope_base) ** np.linspace(0.0, 1.0, DK // 2, dtype=np.float32)
    angle = position[:, None] * inverse[None, :]
    log_gamma = np.log1p(-(2.0 ** (-5.0 - 2.0 * np.arange(4))))
    offset = np.arange(BLOCK)
    distance = offset[:, None] - offset[None, :]
    inside = np.where(distance >= 0, np.exp(log_gamma[:, None, None] * np.maximum(distance, 0)), 0.0)
    query_decay = np.exp(log_gamma[:, None] * (offset + 1.0))
    key_decay = np.exp(log_gamma[:, None] * (BLOCK - 1.0 - offset))
    wide = np.ones((1, 1, BLOCK))
    found = (np.cos(angle), np.sin(angle), inside, query_decay[:, :, None] * wide, key_decay[:, :, None] * wide)
    return tuple(jnp.asarray(t.astype(np.float32)) for t in found)


def layer_kernel(
    resid, mix_gain, q_ref, k_ref, v_ref, head_gain, o_ref, mlp_gain, g_ref, u_ref, d_ref,
    cosine, sine, inside, query_decay, key_decay,
    result,
    wq, wo, wm, wd, other_m, other_d, mixed, rows_in, normed, foreign, proj, heads, state, hidden,
    keep, give, take, both2, take2, sums, back,
    recv, send, local, swap_send, swap_recv, put,
):
    buffers = (wq, wo, wm, wd)
    rep, lo, my, mx, core = (lax.axis_index(a) for a in REP_FS_TP)
    z = rep * 2 + lo
    zu, zd = lax.rem(z + 1, 4), lax.rem(z + 3, 4)
    peers = (
        {"fs_2": lax.rem(mx + 1, 4)},
        {"fs_2": lax.rem(mx + 3, 4)},
        {"fs_1": lax.rem(my + 1, 4)},
        {"fs_1": lax.rem(my + 3, 4)},
        {"rep": zu // 2, "fs_0": lax.rem(zu, 2)},
        {"rep": zd // 2, "fs_0": lax.rem(zd, 2)},
    )
    partner = {"tp": 1 - core}
    barrier = pltpu.get_barrier_semaphore()
    for peer in peers + (partner,):
        pl.semaphore_signal(barrier, inc=1, device_id=peer, device_id_type=MESH_ID)

    def base(offset):
        oz, oy, ox = offset
        owner = (lax.rem(lo + oz, 2) * 4 + lax.rem(my + 4 - oy, 4)) * 4 + lax.rem(mx + 4 - ox, 4)
        return owner * ROWS

    own = pl.ds(pl.multiple_of(base(ROOT), ROWS), ROWS)
    mine = pl.multiple_of(core * HALF, HALF)
    other = pl.multiple_of(HALF - core * HALF, HALF)
    half = (mine, other)

    ze, zb = lax.rem(z + 1 + 2 * core, 4), lax.rem(z + 3 - 2 * core, 4)
    helper = {"rep": ze // 2, "fs_0": lax.rem(ze, 2)}
    helped = {"rep": zb // 2, "fs_0": lax.rem(zb, 2)}

    def columns_of(side, first, count):
        return pl.ds(pl.multiple_of(side * (SIDE + TILE) + first, TILE), count)

    tile, shared = pl.ds(SIDE, TILE), pl.ds(SIDE + FIRST, TILE)
    places = (((0, FIRST), 0, FIRST), ((FIRST, SIDE - FIRST), 2 * FIRST, 2 * FIRST + SIDE - FIRST + TILE))
    parts = {
        0: [(q_ref, wq.at[own, pl.ds(0, 512)]), (k_ref, wq.at[own, pl.ds(512, 512)])],
        1: [(v_ref, wq.at[own, pl.ds(1024, 1024)])],
        2: [(o_ref, wo.at[own, :])],
        3: [],
        4: [(g_ref.at[:, tile], mixed.at[0]), (u_ref.at[:, tile], mixed.at[1])],
        5: [
            (d_ref.at[:, columns_of(lo, 0, SIDE)], wd.at[own, pl.ds(0, SIDE)]),
            (d_ref.at[:, tile], wd.at[own, tile]),
            (d_ref.at[:, columns_of(1 - lo, 0, SIDE)], other_d.at[:, pl.ds(0, SIDE)]),
            (d_ref.at[:, tile], other_d.at[:, tile]),
        ],
    }
    for array, (span, gate_at, up_at) in zip((3, 4), places):
        for ref, at in ((g_ref, gate_at), (u_ref, up_at)):
            there = pl.ds(at, span[1])
            parts[array].append((ref.at[:, columns_of(lo, *span)], wm.at[own, there]))
            parts[array].append((ref.at[:, columns_of(1 - lo, *span)], other_m.at[:, there]))
    fills = {}
    for array, pairs in parts.items():
        fills[array] = []
        for source, there in pairs:
            at = sum(len(f) for f in fills.values())
            fills[array].append(pltpu.make_async_copy(source, there, local.at[at]))
            fills[array][-1].start()
    fill = pltpu.make_async_copy(resid, rows_in.at[pl.ds(mine, HALF), :], local.at[18])
    fill.start()
    pl.semaphore_wait(barrier, 7)

    def swap(source, there, slot, device=partner):
        return pltpu.make_async_remote_copy(
            src_ref=source,
            dst_ref=there,
            send_sem=swap_send.at[0 if slot < 11 else 1],
            recv_sem=swap_recv.at[slot],
            device_id=device,
            device_id_type=MESH_ID,
        )

    swaps = {0: swap(resid, rows_in.at[pl.ds(mine, HALF), :], 0)}
    swaps[0].start()

    def chunk(array, piece, offset):
        buffer, first, width = ARRAYS[array]
        count = ROWS // PIECES[array]
        start = pl.multiple_of(base(offset) + piece * count, count)
        return buffers[buffer].at[pl.ds(start, count), pl.ds(first, width)]

    def key_of(array, piece, offset):
        whole = (array, piece, offset)
        return whole if whole in SLOTS else (array, offset[:2] if array == LAST else None)

    waited = set()

    def arrive(array, piece, offset):
        key = (array,) if offset == ROOT else key_of(array, piece, offset)
        if key in waited:
            return
        waited.add(key)
        if offset == ROOT:
            for item in fills[array]:
                item.wait()
        else:
            buffer, first, width = ARRAYS[array]
            all_rows = COUNTS[key] * ROWS // PIECES[array]
            here = buffers[buffer].at[pl.ds(0, all_rows), pl.ds(first, width)]
            pltpu.make_async_copy(here, here, recv.at[SLOTS[key]]).wait()

    def prepare():
        arrive(4, 0, ROOT)
        lane = lax.broadcasted_iota(jnp.int32, (ROWS, TILE), 1) // (TILE // 2)
        gate = mixed[0].astype(F32)
        up = pltpu.roll(mixed[1].astype(F32), TILE // 2, 1)
        wm[own, shared] = jnp.where(lane == lo, gate, up).astype(BF16)
        other_m[:, shared] = jnp.where(lane == 1 - lo, gate, up).astype(BF16)

    def norm_rows(source, gain, start, count):
        def some(i, _):
            rows = pl.ds(pl.multiple_of(start + i * 32, 32), 32)
            wide = source[rows, :].astype(F32)
            scaled = wide * lax.rsqrt(jnp.mean(wide * wide, axis=-1, keepdims=True) + norm_eps)
            normed[rows, :] = (scaled * gain[...]).astype(BF16)

        lax.fori_loop(0, count // 32, some, None)

    def norm(which):
        if which == 0:
            fill.wait()
        else:
            swaps[0].wait_recv()
        norm_rows(rows_in, mix_gain, half[which], HALF)

    def project(j):
        def some(i, _):
            rows = pl.ds(pl.multiple_of(i * HALF, HALF), HALF)
            columns = pl.ds(256 * j, 256)
            found = jnp.dot(normed[rows, :], wq[:, columns], preferred_element_type=F32).astype(BF16)
            if j < 4:
                wide = found.astype(F32)
                first, second = wide[:, :128], wide[:, 128:]
                c, s = cosine[rows, :], sine[rows, :]
                turned = jnp.concatenate([first * c - second * s, second * c + first * s], axis=1)
                if j >= 2:
                    turned = turned * DK**-0.5
                found = turned.astype(BF16)
            proj[rows, columns] = found

        lax.fori_loop(0, 2, some, None)

    def retain(t, h):
        rows = pl.ds(t * BLOCK, BLOCK)
        head = core * 2 + h
        queries = proj[rows, pl.ds(DK * h, DK)]
        keys = proj[rows, pl.ds(2 * DK + DK * h, DK)]
        values = proj[rows, pl.ds(4 * DK + DV * h, DV)]
        decay = query_decay[head]
        scores = lax.dot_general(queries, keys, (((1,), (1,)), ((), ())), preferred_element_type=F32)
        weights = (scores * inside[head]).astype(BF16)
        found = jnp.dot(weights, values, preferred_element_type=F32)
        if t > 0:
            carried = jnp.dot(queries, state[h].astype(BF16), preferred_element_type=F32)
            found = found + carried * jnp.concatenate([decay] * 4, axis=1)
        if t < LEN // BLOCK - 1:
            fade = key_decay[head]
            faded = (keys.astype(F32) * jnp.concatenate([fade] * 2, axis=1)).astype(BF16)
            fresh = lax.dot_general(faded, values, (((0,), (0,)), ((), ())), preferred_element_type=F32)
            if t > 0:
                last = query_decay[head, BLOCK - 1 : BLOCK, :]
                fresh = state[h] * jnp.concatenate([last] * 4, axis=1) + fresh
            state[h] = fresh
        columns = pl.ds(DV * h, DV)
        scaled = found * lax.rsqrt(jnp.mean(found * found, axis=-1, keepdims=True) + norm_eps)
        heads[rows, columns] = (scaled * head_gain[:, columns]).astype(BF16)

    third = HALF // 3

    def give_heads(which, r):
        rows = pl.ds(pl.multiple_of(half[which] + r * third, third), third)
        there = pl.ds(r * third, third)
        share = give if which else keep

        def some(j, _):
            columns = pl.ds(pl.multiple_of(j * 512, 512), 512)
            share[there, columns] = lax.dot_general(
                heads[rows, :], wo[columns, :], (((1,), (1,)), ((), ())), preferred_element_type=F32
            ).astype(BF16)

        lax.fori_loop(0, 4, some, None)
        if which:
            swaps[35 + r] = swap(give.at[there, :], take.at[there, :], 35 + r)
            swaps[35 + r].start()

    def lend(r):
        here = normed.at[pl.ds(pl.multiple_of(mine + r * third, third), third), :]
        swaps[2 + r] = swap(here, foreign.at[core, pl.ds(r * third, third), :], 2 + r, helper)
        swaps[5 + r] = swap(here, here, 5 + r)
        swaps[2 + r].start()
        swaps[5 + r].start()

    def middle(r):
        swaps[35 + r].wait_recv()

        def some(i, _):
            here = pl.ds(pl.multiple_of(r * third + i * 32, 32), 32)
            rows = pl.ds(pl.multiple_of(mine + r * third + i * 32, 32), 32)
            added = keep[here, :].astype(F32) + take[here, :].astype(F32)
            found = (rows_in[rows, :].astype(F32) + added).astype(BF16)
            rows_in[rows, :] = found
            wide = found.astype(F32)
            scaled = wide * lax.rsqrt(jnp.mean(wide * wide, axis=-1, keepdims=True) + norm_eps)
            normed[rows, :] = (scaled * mlp_gain[...]).astype(BF16)

        lax.fori_loop(0, third // 32, some, None)
        lend(r)

    def forward(i):
        swaps[2 + i].wait_recv()
        here = foreign.at[core, pl.ds(i * third, third), :]
        swaps[8 + i] = swap(here, here, 8 + i)
        swaps[8 + i].start()

    quarter = HALF // 2

    def rows_of(part, i):
        side = core if part % 2 == 0 else 1 - core
        if part < 2:
            source = normed[pl.ds(pl.multiple_of(side * HALF + i * quarter, quarter), quarter), :]
        else:
            source = foreign[side, pl.ds(i * quarter, quarter), :]
        return source, 2 * (part // 2) + side, pl.ds(i * quarter, quarter)

    def expand_first(part, i):
        for r in {(1, 0): (5, 6, 7), (3, 0): (8, 9), (3, 1): (10,)}.get((part, i), ()):
            swaps[r].wait_recv()
        source, place, rows = rows_of(part, i)
        both = jnp.dot(source, wm[:, pl.ds(0, 2 * FIRST)], preferred_element_type=F32)
        hidden[place, rows, pl.ds(0, FIRST)] = (jax.nn.silu(both[:, :FIRST]) * both[:, FIRST:]).astype(BF16)

    def expand_rest(part, i):
        source, place, rows = rows_of(part, i)
        count = SIDE - FIRST
        both = jnp.dot(source, wm[:, pl.ds(2 * FIRST, 2 * count + TILE)], preferred_element_type=F32)
        hidden[place, rows, pl.ds(FIRST, count)] = (
            jax.nn.silu(both[:, :count]) * both[:, count + TILE :]
        ).astype(BF16)
        pair = both[:, count : count + TILE]
        found = jax.nn.silu(pair) * pltpu.roll(pair, TILE // 2, 1)
        lane = lax.broadcasted_iota(jnp.int32, (quarter, TILE), 1) // (TILE // 2)
        hidden[place, rows, tile] = jnp.where(lane == lo, found, 0.0).astype(BF16)
        send_back()

    blocks = {}

    def down_into(g, part, slot):
        block = blocks[g]
        weights = wd.at[pl.ds(pl.multiple_of(block * 256, 256), 256), :]

        def some(i, _):
            side = i * core + (1 - i) * (1 - core)
            both2[block, part, i] = lax.dot_general(
                hidden[2 * part + side], weights[...], (((1,), (1,)), ((), ())), preferred_element_type=F32
            ).astype(BF16)

        lax.fori_loop(0, 2, some, None)
        swaps[slot] = swap(both2.at[block, part, 0], take2.at[block, part], slot)
        swaps[slot].start()

    pending = []

    def send_back():
        for g in pending:
            swaps[11 + g].wait_recv()
            block = blocks[g]

            def some(i, _, block=block):
                rows = pl.ds(pl.multiple_of(i * 96, 32), 96)
                added = both2[block, 1, 1, rows, :].astype(F32) + take2[block, 1, rows, :].astype(F32)
                sums[block, rows, :] = added.astype(BF16)

            lax.fori_loop(0, HALF // 96, some, None)
            swaps[19 + g] = swap(sums.at[block], back.at[block], 19 + g, helped)
            swaps[19 + g].start()
        pending.clear()

    def lent(g):
        oz, oy = GROUPS[g]
        blocks[g] = lax.rem(lo + oz, 2) * 4 + lax.rem(my + 4 - oy, 4)
        down_into(g, 1, 11 + g)
        send_back()
        pending.append(g)

    def own_rows(g):
        down_into(g, 0, 27 + g)
        send_back()
        if g >= 2:
            finish(g - 2)

    def writing(g):
        place = result.at[:, pl.ds(pl.multiple_of(blocks[g] * 256, 256), 256)]
        return pltpu.make_async_copy(both2.at[blocks[g], 0, 1], place, put.at[0])

    def finish(g):
        block = blocks[g]
        swaps[27 + g].wait_recv()
        swap(sums.at[block], back.at[block], 19 + (g ^ 1), helped).wait_recv()

        def some(i, _):
            here = pl.ds(pl.multiple_of(i * 96, 32), 96)
            rows = pl.ds(pl.multiple_of(mine + i * 96, 32), 96)
            columns = pl.ds(pl.multiple_of(block * 256, 256), 256)
            added = both2[block, 0, 1, here, :].astype(F32) + take2[block, 0, here, :].astype(F32)
            added = added + back[block, here, :].astype(F32)
            both2[block, 0, 1, here, :] = (rows_in[rows, columns].astype(F32) + added).astype(BF16)

        lax.fori_loop(0, HALF // 96, some, None)
        writing(g).start()

    run = {
        "prep": prepare, "norm": norm, "proj": project, "ret": retain, "out": give_heads,
        "mid": middle, "pass": forward, "first": expand_first, "rest": expand_rest, "lent": lent, "own": own_rows,
    }
    for name, _, what in ORDER:
        if name == "send":
            d, array, piece, offset, child = what
            arrive(array, piece, offset)
            source = here = chunk(array, piece, offset)
            if array in SPLIT and child == (1, 0, 0):
                buffer, first, width = ARRAYS[array]
                count = ROWS // PIECES[array]
                source = (other_m, other_d)[buffer - 2].at[pl.ds(piece * count, count), pl.ds(first, width)]
            pltpu.make_async_remote_copy(
                src_ref=source,
                dst_ref=here,
                send_sem=send.at[array],
                recv_sem=recv.at[SLOTS[key_of(array, piece, child)]],
                device_id=peers[d],
                device_id_type=MESH_ID,
            ).start()
        else:
            args, wanted = what
            for item in sorted(wanted, key=lambda c: key_of(*c) in COUNTS and COUNTS[key_of(*c)] > 1):
                arrive(*item)
            run[name](*args)
    send_back()
    finish(len(GROUPS) - 2)
    finish(len(GROUPS) - 1)
    for array, (buffer, first, width) in enumerate(ARRAYS):
        sent = buffers[buffer].at[pl.ds(0, 31 * ROWS), pl.ds(first, width)]
        pltpu.make_async_copy(sent, sent, send.at[array]).wait()
    for slot in range(2):
        pltpu.make_async_copy(both2, both2, swap_send.at[slot]).wait()
    pltpu.make_async_copy(result, result, put.at[0]).wait()


def shards(
    resid, mix_gain, query_weight, key_weight, value_weight, head_gain, out_weight, mlp_gain,
    gate_weight, up_weight, down_weight,
):
    anywhere = pl.BlockSpec(memory_space=pl.ANY)
    inside = pl.BlockSpec(memory_space=pltpu.VMEM)
    return pl.pallas_call(
        layer_kernel,
        out_shape=jax.ShapeDtypeStruct((HALF, D), BF16),
        in_specs=[anywhere, inside, anywhere, anywhere, anywhere, inside, anywhere, inside, anywhere, anywhere, anywhere]
        + [inside] * 5,
        out_specs=anywhere,
        scratch_shapes=[
            pltpu.VMEM((D, 2048), BF16),
            pltpu.VMEM((D, 1024), BF16),
            pltpu.VMEM((D, 2 * SIDE + TILE), BF16),
            pltpu.VMEM((D, SIDE + TILE), BF16),
            pltpu.VMEM((ROWS, 2 * SIDE + TILE), BF16),
            pltpu.VMEM((ROWS, SIDE + TILE), BF16),
            pltpu.VMEM((2, ROWS, TILE), BF16),
            pltpu.VMEM((LEN, D), BF16),
            pltpu.VMEM((LEN, D), BF16),
            pltpu.VMEM((2, HALF, D), BF16),
            pltpu.VMEM((LEN, 2048), BF16),
            pltpu.VMEM((LEN, 1024), BF16),
            pltpu.VMEM((2, DK, DV), F32),
            pltpu.VMEM((4, HALF, SIDE + TILE), BF16),
        ]
        + [pltpu.VMEM((HALF, D), BF16)] * 3
        + [pltpu.VMEM((8, 2, 2, HALF, 256), BF16), pltpu.VMEM((8, 2, HALF, 256), BF16)]
        + [pltpu.VMEM((8, HALF, 256), BF16)] * 2
        + [
            pltpu.SemaphoreType.DMA((len(SLOTS),)),
            pltpu.SemaphoreType.DMA((len(ARRAYS),)),
            pltpu.SemaphoreType.DMA((19,)),
            pltpu.SemaphoreType.DMA((2,)),
            pltpu.SemaphoreType.DMA((38,)),
            pltpu.SemaphoreType.DMA((1,)),
        ],
        compiler_params=pltpu.CompilerParams(
            collective_id=0, has_side_effects=True, vmem_limit_bytes=67043328
        ),
    )(
        resid, mix_gain.reshape(1, -1), query_weight, key_weight, value_weight, head_gain.reshape(1, -1),
        out_weight.T, mlp_gain.reshape(1, -1), gate_weight, up_weight, down_weight.T, *tables(),
    )


def solution(mesh):
    torus = Mesh(
        mesh.devices.reshape(mesh.shape["rep"], 2, 4, 4, mesh.shape["tp"]),
        ("rep", "fs_0", "fs_1", "fs_2", "tp"),
    )
    return jax.shard_map(
        shards,
        mesh=torus,
        in_specs=(
            P(REP_FS_TP, None),
            P(),
            P(FS, "tp"),
            P(FS, "tp"),
            P(FS, "tp"),
            P("tp"),
            P("tp", FS),
            P(),
            P(FS, "tp"),
            P(FS, "tp"),
            P("tp", FS),
        ),
        out_specs=P(REP_FS_TP, None),
        check_vma=False,
    )
```
